256 devices in a mesh: sp: 64 (over z, y, core), tp: 4 (over x).
Axes of the slice: x: 4, y: 4, z: 8, core: 2. Of those that a mesh axis runs over, the one named last changes fastest.
Arguments:
- tokens: bfloat16 [16384, 2048], P(('sp', 'tp')), may hold values from -6 to 6
- norm_gain: float32 [2048], replicated, may hold values from 0.1 to 6, as said below
- query_weight: bfloat16 [2048, 16, 128], P(None, 'tp'), may hold values from -0.21875 to 0.21875
- key_weight: bfloat16 [2048, 4, 128], P(None, 'tp'), may hold values from -0.125 to 0.125
- value_weight: bfloat16 [2048, 4, 128], P(None, 'tp'), may hold values from -0.125 to 0.125
- mix_lambda: float32 [16], P('tp'), may hold values from 0.3 to 0.8
- head_gain: float32 [128], replicated, may hold values from 0.1 to 1.9
- pool_weight: bfloat16 [2048, 4, 512], P(None, 'tp'), may hold values from -0.125 to 0.125
- pool_mix: bfloat16 [4, 512, 512], P('tp'), may hold values from -0.25 to 0.25
- pool_scale: float32 [4, 512], P('tp'), may hold values from 0.1 to 1.9
- gate_weight: bfloat16 [2048, 2, 2048], P(None, None, 'tp'), may hold values from -0.125 to 0.125
- out_weight: bfloat16 [2048, 2048], P('tp'), may hold values from -0.125 to 0.125
Outputs:
- mixed: bfloat16 [16384, 2048], P(('sp', 'tp'))
- log_sums: float32 [2, 16, 16384], P(None, 'tp', 'sp')
The draws below stay inside these ranges and needn't reach their ends.
Inputs may be any that keep to these rules, and one draw needn't show every extreme that they name: `norm_gain`: positive.
All inputs are finite; a program needn't handle non-finite values.
Results may differ from the reference program's by a relative error of at most 0.013.
Values may be sent and summed in bfloat16 or wider, within the bound.
A program may use at most 128 MiB of HBM per device.

```python
import math
import jax
import jax.numpy as jnp
from jax import lax

D = 2048
HEADS = 16
HD = 64
DV = 128
KV_HEADS = 4
GROUPS = 4
GW = 512
WINDOW = 16
TOKENS = 16384
N_TP = 4


def draw_norm_gain(key, part):
    return 1.0 + 0.18 * jnp.clip(jax.random.normal(key, (D,), jnp.float32), -5.0, 5.0)


def block_levels(stream_key, extent, shards, least, largest):
    factor_of = 1.0
    for dim, parts in shards:
        draws = jax.random.uniform(jax.random.fold_in(jax.random.fold_in(stream_key, 6), dim), (parts,), jnp.float32, least / len(shards), largest / len(shards))
        factor_of = factor_of * jnp.repeat(jnp.exp(draws), extent[dim] // parts).reshape((-1,) + (1,) * (len(extent) - 1 - dim))
    return factor_of


def bell_draw(own_key, dims, width, most, cuts=(), held_as=jnp.bfloat16):
    values = width * jax.random.normal(own_key, dims, jnp.float32)
    if cuts:
        values = values * block_levels(own_key, dims, cuts, -0.22, 0.18)
    return jnp.clip(values, -most, most).astype(held_as)


def setup_inputs(seed: int = 0) -> dict:
    key_list = jax.random.split(jax.random.key(seed), 13)
    return {
        "tokens": bell_draw(key_list[0], (TOKENS, D), 1.0, 6.0, ((0, 256),)),
        "norm_gain": draw_norm_gain(jax.random.fold_in(key_list[12], 71), 0),
        "query_weight": bell_draw(key_list[2], (D, HEADS, 2 * HD), (D // 3) ** -0.5, 0.21875, ((1, 4),)),
        "key_weight": bell_draw(key_list[3], (D, KV_HEADS, 2 * HD), D ** -0.5, 0.125, ((1, 4),)),
        "value_weight": bell_draw(key_list[4], (D, KV_HEADS, DV), D ** -0.5, 0.125, ((1, 4),)),
        "mix_lambda": jnp.clip(0.3 + 0.5 * jax.random.uniform(key_list[5], (HEADS,), jnp.float32) ** block_levels(key_list[5], (HEADS,), ((0, 4),), -0.2, 0.2), 0.3, 0.8),
        "head_gain": jnp.clip(1.0 + 0.18 * jax.random.normal(key_list[6], (DV,), jnp.float32), 0.1, 1.9),
        "pool_weight": bell_draw(key_list[7], (D, GROUPS, GW), D ** -0.5, 0.125, ((1, 4),)),
        "pool_mix": bell_draw(key_list[8], (GROUPS, GW, GW), GW ** -0.5, 0.25, ((0, 4),)),
        "pool_scale": jnp.clip(1.0 + 0.18 * jax.random.normal(key_list[9], (GROUPS, GW), jnp.float32), 0.1, 1.9),
        "gate_weight": bell_draw(key_list[10], (D, 2, D), D ** -0.5, 0.125, ((2, 4),)),
        "out_weight": bell_draw(key_list[11], (D, D), D ** -0.5, 0.125, ((0, 4),)),
    }


NORM_EPS = 1e-06

def reference(tokens, norm_gain, query_weight, key_weight, value_weight, mix_lambda, head_gain, pool_weight, pool_mix, pool_scale, gate_weight, out_weight):
    inputs = tokens.astype(jnp.float32)
    normed = (inputs * lax.rsqrt(lax.optimization_barrier(jnp.mean(inputs * inputs, axis=1, keepdims=True)) + NORM_EPS) * norm_gain).astype(jnp.bfloat16)

    def project(weight):
        return jnp.dot(normed, weight.reshape(D, -1), preferred_element_type=jnp.float32).astype(jnp.bfloat16)
    queries = project(query_weight).reshape(TOKENS, HEADS, 2, HD)
    keys_all = project(key_weight).reshape(TOKENS, KV_HEADS, 2, HD)
    values_all = project(value_weight).reshape(TOKENS, KV_HEADS, DV)
    pool_in = project(pool_weight).reshape(TOKENS, GROUPS, GW)
    gate_pre = project(gate_weight).reshape(TOKENS, 2, D)
    group_size = HEADS // KV_HEADS
    block_rows = math.gcd(TOKENS, 1024)
    positions = jnp.arange(TOKENS, dtype=jnp.int32)
    score_scale = HD ** (-0.5)

    def one_head(head_index):
        kv_index = head_index // group_size
        head_queries = lax.dynamic_index_in_dim(queries, head_index, 1, keepdims=False).astype(jnp.float32)
        head_keys = lax.dynamic_index_in_dim(keys_all, kv_index, 1, keepdims=False).astype(jnp.float32)
        head_values = lax.dynamic_index_in_dim(values_all, kv_index, 1, keepdims=False)
        weight_lambda = lax.dynamic_index_in_dim(mix_lambda, head_index, 0, keepdims=False)

        def one_block(block_index):
            first_row = block_index * block_rows
            block_queries = lax.dynamic_slice_in_dim(head_queries, first_row, block_rows, 0)
            query_pos = first_row + jnp.arange(block_rows, dtype=jnp.int32)
            scores = jnp.einsum('qmd,kmd->mqk', block_queries, head_keys) * score_scale
            causal = positions[None, None, :] <= query_pos[None, :, None]
            masked = jnp.where(causal, scores, -jnp.inf)
            row_top = lax.optimization_barrier(jnp.max(masked, axis=2, keepdims=True))
            probs = jnp.exp(masked - row_top)
            row_sum = lax.optimization_barrier(jnp.sum(probs, axis=2, keepdims=True))
            log_total = row_top + jnp.log(row_sum)
            probs_low = probs.astype(jnp.bfloat16)
            first_map = jnp.dot(probs_low[0], head_values, preferred_element_type=jnp.float32)
            second_map = jnp.dot(probs_low[1], head_values, preferred_element_type=jnp.float32)
            block_out = first_map / row_sum[0] - weight_lambda * (second_map / row_sum[1])
            return (block_out, log_total[:, :, 0])
        outs, logs = lax.map(one_block, jnp.arange(TOKENS // block_rows, dtype=jnp.int32))
        return (outs.reshape(TOKENS, DV), jnp.transpose(logs, (1, 0, 2)).reshape(2, TOKENS))
    head_outs, head_logs = lax.map(one_head, jnp.arange(HEADS, dtype=jnp.int32))
    normed_heads = head_outs * lax.rsqrt(lax.optimization_barrier(jnp.mean(head_outs * head_outs, axis=2, keepdims=True)) + NORM_EPS) * head_gain
    attended = jnp.transpose(normed_heads, (1, 0, 2)).reshape(TOKENS, D)
    extended = jnp.concatenate([jnp.zeros((WINDOW, GROUPS, GW), jnp.float32), pool_in.astype(jnp.float32)], axis=0)
    group_parts = []
    for group_index in range(GROUPS):
        window_span = 2 ** (group_index + 1)
        window_sum = jnp.zeros((TOKENS, GW), jnp.float32)
        for back_rows in range(window_span):
            window_sum = window_sum + extended[WINDOW - back_rows:WINDOW - back_rows + TOKENS, group_index]
        counts = jnp.minimum(positions + 1, window_span).astype(jnp.float32)
        means = window_sum / counts[:, None]
        pooled = (means - pool_in[:, group_index].astype(jnp.float32)).astype(jnp.bfloat16)
        group_parts.append(jnp.dot(pooled, pool_mix[group_index], preferred_element_type=jnp.float32) * pool_scale[group_index])
    pool_out = jnp.concatenate(group_parts, axis=1)
    merged = (jax.nn.sigmoid(gate_pre[:, 0].astype(jnp.float32)) * attended + jax.nn.sigmoid(gate_pre[:, 1].astype(jnp.float32)) * pool_out).astype(jnp.bfloat16)
    block_cols = D // N_TP
    out_total = jnp.zeros((TOKENS, D), jnp.float32)
    for part_index in range(N_TP):
        partial_out = jnp.dot(merged[:, part_index * block_cols:(part_index + 1) * block_cols], out_weight[part_index * block_cols:(part_index + 1) * block_cols], preferred_element_type=jnp.float32).astype(jnp.bfloat16)
        out_total = out_total + lax.optimization_barrier(partial_out).astype(jnp.float32)
    return (out_total.astype(jnp.bfloat16), jnp.transpose(head_logs, (1, 0, 2)))
```

```python
import functools

import jax
import jax.numpy as jnp
from jax import lax
from jax.experimental import pallas as pl
from jax.experimental.pallas import tpu as pltpu
from jax.sharding import PartitionSpec as P

WINDOW = 16
NORM_EPS = 1e-06
MESH = pl.DeviceIdType.MESH
NEG = -1e30
NZ, NY, NC = 8, 4, 2
LAG, NB = 2, 4
ROWS = 256
HALF = 128
KB = 512


def copy_for_each(array, axis):
    size = lax.axis_size(axis)
    return lax.all_to_all(
        jnp.broadcast_to(array[None], (size, *array.shape)), axis, 0, 0, tiled=True
    )


def shifted(block, axis, distance):
    devices = range(lax.axis_size(axis))
    route = [(i - distance, i) for i in devices if i - distance in devices]
    return lax.ppermute(block, axis, route)


def sent_and_summed(array, axis):
    size = lax.axis_size(axis)
    pieces = lax.all_to_all(array.reshape(size, -1, array.shape[1]), axis, 0, 0, tiled=True)
    return jnp.sum(pieces.astype(jnp.float32), axis=0)


def attention_kernel(
    q_ref, qs_ref, k_ref, v_ref, lam_ref, gain_ref,
    att_ref, lse_ref,
    gk, gv, qbd, qin, m_ref, acc_ref, attx, lsex, attr, lser,
    *rest,
):
    sb, pb, bm = rest[:NB], rest[NB:2 * NB], rest[2 * NB:3 * NB]
    (own_sem, ky_s, ky_r, vy_s, vy_r, kz_s, kz_r, vz_s, vz_r,
     sk_s, sk_r, sv_s, sv_r, q_s, q_r, o_s, o_r) = rest[3 * NB:]
    me = lax.axis_index("sp")
    z, y, c = me // (NY * NC), (me // NC) % NY, me % NC

    def at(zz, yy, cc):
        return {"sp": (zz * NY + yy) * NC + cc}

    sibling = at(z, y, 1 - c)
    partner = at(NZ - 1 - z, NY - 1 - y, c)
    z_up, z_down = at((z + 1) % NZ, y, c), at((z + NZ - 1) % NZ, y, c)
    y_peers = [at(z, (y + d) % NY, c) for d in (1, 2, 3)]

    barrier = pltpu.get_barrier_semaphore()
    peers = [sibling, partner, z_up, z_down, *y_peers]
    for peer in peers:
        pl.semaphore_signal(barrier, inc=1, device_id=peer, device_id_type=MESH)
    pl.semaphore_wait(barrier, len(peers))

    def remote(src, dst, s, r, dev):
        return pltpu.make_async_remote_copy(
            src_ref=src, dst_ref=dst, send_sem=s, recv_sem=r,
            device_id=dev, device_id_type=MESH,
        )

    def slab(j):
        k = (j + 1) // 2
        return lax.rem(z + NZ + jnp.where(lax.rem(j, 2) == 1, -k, k), NZ)

    def k_to_y(j, d):
        zs = slab(j)
        return remote(gk.at[zs, c, y], gk.at[zs, c, y], ky_s.at[j, d], ky_r.at[j, d], y_peers[d])

    def k_from_y(j, d):
        zs, yy = slab(j), lax.rem(y + NY - (d + 1), NY)
        return remote(gk.at[zs, c, yy], gk.at[zs, c, yy], ky_s.at[j, d], ky_r.at[j, d], y_peers[d])

    def v_to_y(d):
        return remote(v_ref, gv.at[z, c, y], vy_s.at[d], vy_r.at[d], y_peers[d])

    def v_from_y(d):
        yy = lax.rem(y + NY - (d + 1), NY)
        return remote(v_ref, gv.at[z, c, yy], vy_s.at[d], vy_r.at[d], y_peers[d])

    def to_z(j, zs):
        dev = {"sp": jnp.where(lax.rem(j, 2) == 1, z_up["sp"], z_down["sp"])}
        return (
            remote(gk.at[zs, c, y], gk.at[zs, c, y], kz_s.at[j], kz_r.at[j], dev),
            remote(gv.at[zs, c], gv.at[zs, c], vz_s.at[j], vz_r.at[j], dev),
        )

    def to_sibling(j, cc):
        zs = slab(j)
        return (
            remote(gk.at[zs, cc], gk.at[zs, cc], sk_s.at[j], sk_r.at[j], sibling),
            remote(gv.at[zs, cc], gv.at[zs, cc], sv_s.at[j], sv_r.at[j], sibling),
        )

    q_copy = remote(qs_ref, qin, q_s, q_r, partner)
    q_copy.start()
    own_k = pltpu.make_async_copy(k_ref, gk.at[z, c, y], own_sem.at[0])
    own_v = pltpu.make_async_copy(v_ref, gv.at[z, c, y], own_sem.at[1])
    own_k.start()
    own_v.start()
    for d in range(3):
        v_to_y(d).start()
    own_k.wait()
    for d in range(3):
        k_to_y(0, d).start()
    own_v.wait()

    m_ref[...] = jnp.full_like(m_ref, NEG)
    acc_ref[...] = jnp.zeros_like(acc_ref)
    is_low = z < NZ // 2
    g_own = jnp.where(is_low, 0, 4)
    g_far = 4 - g_own

    def block_diagonal(q):
        top = lax.broadcasted_iota(jnp.int32, (HALF, HALF), 0) < 64
        zero = jnp.zeros_like(q)
        return jnp.concatenate([jnp.where(top, q, zero), jnp.where(top, zero, q)], axis=1)

    for h in range(4):
        qbd[g_own + h] = block_diagonal(q_ref[h])

    for d in range(3):
        v_from_y(d).wait_recv()
    for j in (1, 2):
        for copy in to_z(j, z):
            copy.start()

    def stage1(j):
        zs = slab(j)
        for copy in to_z(j, zs):
            copy.wait_recv()

        @pl.when(j <= 5)
        def _():
            for copy in to_z(j + 2, zs):
                copy.start()

        for d in range(3):
            k_to_y(j, d).start()

    def stage2(j):
        for d in range(3):
            k_from_y(j, d).wait_recv()
        for copy in to_sibling(j, c):
            copy.start()

    def stage3(j):
        for copy in to_sibling(j, 1 - c):
            copy.wait_recv()

    chip = z * NY + y
    lo = jnp.minimum(chip, 31 - chip)
    hi = 31 - lo

    ones = jnp.ones((16, KB), jnp.bfloat16)

    def keys(i):
        zs, yy = i // NY, lax.rem(i, NY)
        return jnp.concatenate([gk[zs, 0, yy], gk[zs, 1, yy]], axis=0)

    def values(i):
        zs, yy = i // NY, lax.rem(i, NY)
        v0, v1 = gv[zs, 0, yy], gv[zs, 1, yy]
        vt = jnp.concatenate([v0[:HALF], v0[HALF:], v1[:HALF], v1[HALF:]], axis=1)
        return jnp.concatenate([vt, ones], axis=0)

    def scores(i, t, slot, base=None):
        s = jnp.dot(keys(i), qbd[t], preferred_element_type=jnp.float32)
        if base is not None:
            key_pos = i * KB + lax.broadcasted_iota(jnp.int32, (KB, 2 * HALF), 0)
            row = lax.broadcasted_iota(jnp.int32, (KB, 2 * HALF), 1)
            row_pos = base + jnp.where(row < HALF, row, row - HALF)
            s = jnp.where(key_pos <= row_pos, s, NEG)
        sb[slot][...] = s
        bm[slot][...] = jnp.max(s, axis=0, keepdims=True)

    def weigh(i, t, slot):
        old = m_ref[t]
        new = jnp.maximum(old, bm[slot][...])
        m_ref[t] = new
        pb[slot][...] = jnp.exp(sb[slot][...] - new).astype(jnp.bfloat16)
        acc_ref[t] = acc_ref[t] * jnp.exp(old - new) + jnp.dot(
            values(i), pb[slot][...], preferred_element_type=jnp.float32
        )

    def sweep(begin, end, tiles):
        n = len(tiles)

        @pl.when(begin < end)
        def _():
            for u in range(LAG):
                scores(begin, tiles[u], u % NB)

            def step(i, carry):
                nxt = jnp.minimum(i + 1, end - 1)
                for u in range(n):
                    ahead = u + LAG
                    scores(i if ahead < n else nxt, tiles[ahead % n], ahead % NB)
                    weigh(i, tiles[u], u % NB)
                return carry

            lax.fori_loop(begin, end, step, 0)

    def masked(i, first, base):
        for u in range(LAG):
            scores(i, first + u, u % NB, base)
        for u in range(4):
            if u + LAG < 4:
                scores(i, first + u + LAG, (u + LAG) % NB, base)
            weigh(i, first + u, u % NB)

    p_own = me * ROWS
    p_far = partner["sp"] * ROWS + HALF
    base_lo = jnp.where(is_low, p_own, p_far)
    base_hi = jnp.where(is_low, p_far, p_own)

    def compute(j):
        zs = slab(j)
        first, last = zs * NY, zs * NY + NY
        sweep(first, jnp.minimum(last, lo), list(range(8)))
        sweep(jnp.maximum(first, lo), jnp.minimum(last, hi), list(range(4, 8)))
        in_lo = lo // NY == zs
        in_hi = hi // NY == zs

        def diagonal(g, carry):
            @pl.when(jnp.where(g == 0, in_lo, in_hi))
            def _():
                masked(jnp.where(g == 0, lo, hi), g * 4, jnp.where(g == 0, base_lo, base_hi))
            return carry

        lax.fori_loop(0, 2, diagonal, 0)

    stage1(1)
    stage2(0)
    q_copy.wait_recv()
    for h in range(4):
        qbd[g_far + h] = block_diagonal(qin[h])

    def per_slab(j, carry):
        @pl.when(j <= 5)
        def _():
            stage1(j + 2)

        @pl.when(j <= 6)
        def _():
            stage2(j + 1)

        stage3(j)
        compute(j)
        return carry

    lax.fori_loop(0, NZ, per_slab, 0)

    def finish(group, att_out, lse_out):
        for h in range(4):
            acc = acc_ref[group + h]
            m = m_ref[group + h]
            total = acc[HALF:HALF + 1]
            lse = m + jnp.log(total)
            lse_out[0, h:h + 1, :] = lse[:, :HALF]
            lse_out[1, h:h + 1, :] = lse[:, HALF:]
            both = acc[:HALF] / total
            out = both[:, :HALF] - lam_ref[h:h + 1, :] * both[:, HALF:]
            scale = lax.rsqrt(jnp.mean(out * out, axis=0, keepdims=True) + NORM_EPS)
            normed = out * scale * gain_ref[...]
            att_out[:, h * HALF:(h + 1) * HALF] = normed.T.astype(jnp.bfloat16)

    finish(g_far, attx, lsex)
    finish(g_own, att_ref.at[0], lse_ref.at[0])
    back = (remote(attx, attr, o_s.at[0], o_r.at[0], partner),
            remote(lsex, lser, o_s.at[1], o_r.at[1], partner))
    for copy in back:
        copy.start()

    q_copy.wait_send()
    for d in range(3):
        v_to_y(d).wait_send()

    def drain(j, carry):
        for d in range(3):
            k_to_y(j, d).wait_send()
        for copy in to_sibling(j, c):
            copy.wait_send()
        return carry

    lax.fori_loop(0, NZ, drain, 0)

    def drain_z(j, carry):
        for copy in to_z(j, z):
            copy.wait_send()
        return carry

    lax.fori_loop(1, NZ, drain_z, 0)
    for copy in back:
        copy.wait()
    att_ref[1] = attr[...]
    lse_ref[1] = lser[...]


def attend(queries, keys_own, values_own, lam, head_gain):
    qt = jnp.transpose(queries * jnp.asarray(0.125, jnp.bfloat16), (1, 2, 0))
    vt = values_own.reshape(2, HALF, 128).transpose(0, 2, 1).reshape(ROWS, 128)
    bf, f32 = jnp.bfloat16, jnp.float32
    dma = pltpu.SemaphoreType.DMA
    vmem = pl.BlockSpec(memory_space=pltpu.VMEM)
    return pl.pallas_call(
        attention_kernel,
        out_shape=(
            jax.ShapeDtypeStruct((2, HALF, 512), bf),
            jax.ShapeDtypeStruct((2, 2, 4, HALF), f32),
        ),
        in_specs=[vmem] * 6,
        out_specs=(vmem, vmem),
        scratch_shapes=[
            pltpu.VMEM((NZ, NC, NY, ROWS, 128), bf),
            pltpu.VMEM((NZ, NC, NY, ROWS, 128), bf),
            pltpu.VMEM((8, 128, 256), bf),
            pltpu.VMEM((4, 128, 128), bf),
            pltpu.VMEM((8, 1, 256), f32),
            pltpu.VMEM((8, 144, 256), f32),
            pltpu.VMEM((HALF, 512), bf),
            pltpu.VMEM((2, 4, HALF), f32),
            pltpu.VMEM((HALF, 512), bf),
            pltpu.VMEM((2, 4, HALF), f32),
            *[pltpu.VMEM((KB, 256), f32)] * NB,
            *[pltpu.VMEM((KB, 256), bf)] * NB,
            *[pltpu.VMEM((1, 256), f32)] * NB,
            dma((2,)),
            dma((8, 3)), dma((8, 3)), dma((3,)), dma((3,)),
            dma((8,)), dma((8,)), dma((8,)), dma((8,)),
            dma((8,)), dma((8,)), dma((8,)), dma((8,)),
            dma, dma, dma((2,)), dma((2,)),
        ],
        compiler_params=pltpu.CompilerParams(
            collective_id=0, has_side_effects=True, vmem_limit_bytes=48 * 2**20
        ),
        name="attend",
    )(
        qt[:, :, :HALF], qt[:, :, HALF:], keys_own, vt,
        jnp.broadcast_to(lam[:, None], (4, HALF)),
        jnp.broadcast_to(head_gain[:, None], (128, HALF)),
    )


def local(
    tokens,
    norm_gain,
    query_weight,
    key_weight,
    value_weight,
    mix_lambda,
    head_gain,
    pool_weight,
    pool_mix,
    pool_scale,
    gate_weight,
    out_weight,
):
    model_width = tokens.shape[1]
    heads_local = query_weight.shape[1]
    group_width = pool_weight.shape[2]
    channels = gate_weight.shape[2]
    matrices = (
        query_weight.reshape(model_width, -1),
        key_weight.reshape(model_width, -1),
        value_weight.reshape(model_width, -1),
        pool_weight.reshape(model_width, -1),
        gate_weight.reshape(model_width, -1),
    )
    rows = copy_for_each(tokens, "tp").reshape(-1, model_width)
    inputs = rows.astype(jnp.float32)
    normed = (
        inputs
        * lax.rsqrt(jnp.mean(inputs * inputs, axis=1, keepdims=True) + NORM_EPS)
        * norm_gain
    ).astype(jnp.bfloat16)
    queries, keys_own, values_own, pool_in, gate_pre = [
        jnp.dot(normed, matrix, preferred_element_type=jnp.float32).astype(jnp.bfloat16)
        for matrix in matrices
    ]
    tok_rows = rows.shape[0]
    rim_prev = shifted(pool_in[tok_rows - WINDOW :], "sp", 1)
    att, lse = attend(
        queries.reshape(tok_rows, heads_local, 128), keys_own, values_own, mix_lambda, head_gain
    )
    attended = att.reshape(tok_rows, 512).astype(jnp.float32)
    log_out = jnp.concatenate([lse[0], lse[1]], axis=2)
    gate_pre = gate_pre.reshape(tok_rows, 2, channels)
    positions = lax.axis_index("sp") * tok_rows + jnp.arange(tok_rows, dtype=jnp.int32)
    extended = jnp.concatenate([rim_prev, pool_in], axis=0).astype(jnp.float32)
    window_span = jnp.left_shift(jnp.int32(2), lax.axis_index("tp"))
    window_sum = jnp.zeros((tok_rows, group_width), jnp.float32)
    for back_rows in range(WINDOW):
        window_sum = window_sum + jnp.where(
            back_rows < window_span,
            extended[WINDOW - back_rows : WINDOW - back_rows + tok_rows],
            0.0,
        )
    counts = jnp.minimum(positions + 1, window_span).astype(jnp.float32)
    means = window_sum / counts[:, None]
    pooled = (means - pool_in.astype(jnp.float32)).astype(jnp.bfloat16)
    group_parts = jnp.dot(pooled, pool_mix[0], preferred_element_type=jnp.float32) * pool_scale[0]
    merged = (
        jax.nn.sigmoid(gate_pre[:, 0].astype(jnp.float32)) * attended
        + jax.nn.sigmoid(gate_pre[:, 1].astype(jnp.float32)) * group_parts
    ).astype(jnp.bfloat16)
    mixed = sent_and_summed(
        jnp.dot(merged, out_weight, preferred_element_type=jnp.float32).astype(jnp.bfloat16),
        "tp",
    )
    return (mixed.astype(jnp.bfloat16), log_out)


def solution(mesh):
    in_specs = (
        P(("sp", "tp"), None),
        P(),
        P(None, "tp", None),
        P(None, "tp", None),
        P(None, "tp", None),
        P("tp"),
        P(),
        P(None, "tp", None),
        P("tp", None, None),
        P("tp", None),
        P(None, None, "tp"),
        P("tp", None),
    )
    out_specs = (P(("sp", "tp"), None), P(None, "tp", "sp"))
    return jax.shard_map(local, mesh=mesh, in_specs=in_specs, out_specs=out_specs, check_vma=False)
```

```python
import functools

import jax
import jax.numpy as jnp
from jax import lax
from jax.experimental import pallas as pl
from jax.experimental.pallas import tpu as pltpu
from jax.sharding import PartitionSpec as P

WINDOW = 16
NORM_EPS = 1e-06
MESH = pl.DeviceIdType.MESH
NEG = -1e30
NZ, NY, NC = 8, 4, 2
LAG, NB = 3, 4
ROWS = 256
HALF = 128
KB = 1024


def copy_for_each(array, axis):
    size = lax.axis_size(axis)
    return lax.all_to_all(
        jnp.broadcast_to(array[None], (size, *array.shape)), axis, 0, 0, tiled=True
    )


def shifted(block, axis, distance):
    devices = range(lax.axis_size(axis))
    route = [(i - distance, i) for i in devices if i - distance in devices]
    return lax.ppermute(block, axis, route)


def sent_and_summed(array, axis):
    size = lax.axis_size(axis)
    pieces = lax.all_to_all(array.reshape(size, -1, array.shape[1]), axis, 0, 0, tiled=True)
    return jnp.sum(pieces.astype(jnp.float32), axis=0)


def attention_kernel(
    q_ref, qs_ref, k_ref, v_ref, lam_ref, gain_ref,
    att_ref, lse_ref,
    kv, qbd, qin, m_ref, acc_ref, attx, lsex, attr, lser,
    *rest,
):
    sb, pb, bm = rest[:NB], rest[NB:2 * NB], rest[2 * NB:3 * NB]
    (own_sem, y_s, y_r, vy_s, vy_r, z_s, z_r,
     sib_s, sib_r, q_s, q_r, o_s, o_r) = rest[3 * NB:]
    me = lax.axis_index("sp")
    z, y, c = me // (NY * NC), (me // NC) % NY, me % NC

    def at(zz, yy, cc):
        return {"sp": (zz * NY + yy) * NC + cc}

    sibling = at(z, y, 1 - c)
    partner = at(NZ - 1 - z, NY - 1 - y, c)
    z_next = [at((z + 1) % NZ, y, c), at((z + NZ - 1) % NZ, y, c)]
    y_peers = [at(z, (y + d) % NY, c) for d in (1, 2, 3)]

    barrier = pltpu.get_barrier_semaphore()
    peers = [sibling, partner, *z_next, *y_peers]
    for peer in peers:
        pl.semaphore_signal(barrier, inc=1, device_id=peer, device_id_type=MESH)
    pl.semaphore_wait(barrier, len(peers))

    def remote(src, dst, s, r, dev):
        return pltpu.make_async_remote_copy(
            src_ref=src, dst_ref=dst, send_sem=s, recv_sem=r,
            device_id=dev, device_id_type=MESH,
        )

    def slab(k, way):
        return lax.rem(z + NZ + (k if way else -k), NZ)

    def k_to_y(k, way, d):
        piece = kv.at[slab(k, way), c, 0, y]
        return remote(piece, piece, y_s.at[way, k, d], y_r.at[way, k, d], y_peers[d])

    def k_from_y(k, way, d):
        piece = kv.at[slab(k, way), c, 0, lax.rem(y + NY - (d + 1), NY)]
        return remote(piece, piece, y_s.at[way, k, d], y_r.at[way, k, d], y_peers[d])

    def v_to_y(d):
        return remote(v_ref, kv.at[z, c, 1, y], vy_s.at[d], vy_r.at[d], y_peers[d])

    def v_from_y(d):
        yy = lax.rem(y + NY - (d + 1), NY)
        return remote(v_ref, kv.at[z, c, 1, yy], vy_s.at[d], vy_r.at[d], y_peers[d])

    def z_piece(zs, r):
        kind = jnp.minimum(r, 1)
        return kv.at[zs, c, kind, lax.rem(y + jnp.maximum(r - 1, 0), NY)]

    def z_msg(k, r, way, src_k, src=None):
        piece = z_piece(slab(src_k, way), r)
        return remote(
            piece if src is None else src, piece,
            z_s.at[way, k, r], z_r.at[way, k, r], z_next[way],
        )

    def to_sibling(k, way, cc):
        part = kv.at[slab(k, way), cc]
        return remote(part, part, sib_s.at[way, k], sib_r.at[way, k], sibling)

    own_k = pltpu.make_async_copy(k_ref, kv.at[z, c, 0, y], own_sem.at[0])
    own_v = pltpu.make_async_copy(v_ref, kv.at[z, c, 1, y], own_sem.at[1])
    own_k.start()
    own_v.start()
    for d in (0, 2, 1):
        v_to_y(d).start()
    for way in (0, 1):
        z_msg(1, 0, way, 0, k_ref).start()
        z_msg(1, 1, way, 0, v_ref).start()
    q_copy = remote(qs_ref, qin, q_s, q_r, partner)
    q_copy.start()
    own_k.wait()
    for d in (0, 2, 1):
        k_to_y(0, 0, d).start()
    own_v.wait()

    m_ref[...] = jnp.full_like(m_ref, NEG)
    acc_ref[...] = jnp.zeros_like(acc_ref)
    is_low = z < NZ // 2
    g_own = jnp.where(is_low, 0, 4)
    g_far = 4 - g_own

    def block_diagonal(q):
        top = lax.broadcasted_iota(jnp.int32, (HALF, HALF), 0) < 64
        zero = jnp.zeros_like(q)
        return jnp.concatenate([jnp.where(top, q, zero), jnp.where(top, zero, q)], axis=1)

    for h in range(4):
        qbd[g_own + h] = block_diagonal(q_ref[h])

    for r in (2, 4, 3):
        v_from_y(NY - r).wait_recv()
        for way in (0, 1):
            z_msg(1, r, way, 0).start()

    mine = (z * NY + y) // 2
    lo = jnp.minimum(mine, 15 - mine)
    hi = 15 - lo

    ones = jnp.ones((16, KB), jnp.bfloat16)

    def pieces(i, kind):
        zs, yy = i // 2, 2 * lax.rem(i, 2)
        return [kv[zs, cc, kind, yy + d] for d in (0, 1) for cc in (0, 1)]

    def keys(i):
        return jnp.concatenate(pieces(i, 0), axis=0)

    def values(i):
        halves = [v[a:a + HALF] for v in pieces(i, 1) for a in (0, HALF)]
        return jnp.concatenate([jnp.concatenate(halves, axis=1), ones], axis=0)

    def scores(i, t, slot, base=None):
        s = jnp.dot(keys(i), qbd[t], preferred_element_type=jnp.float32)
        if base is not None:
            key_pos = i * KB + lax.broadcasted_iota(jnp.int32, (KB, 2 * HALF), 0)
            row = lax.broadcasted_iota(jnp.int32, (KB, 2 * HALF), 1)
            row_pos = base + jnp.where(row < HALF, row, row - HALF)
            s = jnp.where(key_pos <= row_pos, s, NEG)
        sb[slot][...] = s
        bm[slot][...] = jnp.max(s, axis=0, keepdims=True)

    def weigh(i, t, slot):
        old = m_ref[t]
        new = jnp.maximum(old, bm[slot][...])
        m_ref[t] = new
        pb[slot][...] = jnp.exp(sb[slot][...] - new).astype(jnp.bfloat16)
        acc_ref[t] = acc_ref[t] * jnp.exp(old - new) + jnp.dot(
            values(i), pb[slot][...], preferred_element_type=jnp.float32
        )

    def block(i, tiles, base=None):
        n = len(tiles)
        for u in range(LAG):
            scores(i, tiles[u], u % NB, base)
        for u in range(n):
            if u + LAG < n:
                scores(i, tiles[u + LAG], (u + LAG) % NB, base)
            weigh(i, tiles[u], u % NB)

    p_own = me * ROWS
    p_far = partner["sp"] * ROWS + HALF
    base_lo = jnp.where(is_low, p_own, p_far)
    base_hi = jnp.where(is_low, p_far, p_own)

    def compute(i):
        @pl.when(i < lo)
        def _():
            block(i, list(range(8)))

        @pl.when((i >= lo) & (i < hi))
        def _():
            block(i, list(range(4, 8)))

        @pl.when((i == lo) | (i == hi))
        def _():
            first = jnp.where(i == lo, 0, 4)
            block(i, [first + u for u in range(4)], jnp.where(i == lo, base_lo, base_hi))

    def share(k, ways):
        for way in ways:
            for d in range(3):
                k_from_y(k, way, d).wait_recv()
            to_sibling(k, way, c).start()

    def shared(k, ways):
        for way in ways:
            to_sibling(k, way, 1 - c).wait_recv()

    def serve(k, r, way, forward):
        z_msg(k, r, way, k).wait_recv()
        if forward is not None:
            @pl.when(forward)
            def _():
                z_msg(k + 1, r, way, k).start()

        @pl.when(r == 0)
        def _():
            for d in (0, 2, 1):
                k_to_y(k, way, d).start()

    def both(k, r):
        serve(k, r, 0, (k < 3) | (r <= 2))
        serve(k, r, 1, (k < 3) | (r >= 3))

    def tick(n, carry):
        k, r = n // 5 + 1, lax.rem(n, 5)

        @pl.when(k <= 3)
        def _():
            both(k, r)

        @pl.when((k == 4) & (r <= 2))
        def _():
            serve(k, r, 0, None)

        @pl.when((k == 4) & (r <= 1))
        def _():
            z_msg(k, r + 3, 1, k).wait_recv()

        @pl.when((r == 4) & (k <= 3))
        def _():
            share(k, (0, 1))

        @pl.when(r == 1)
        def _():
            shared(k - 1, (0,))

            @pl.when(k > 1)
            def _():
                shared(k - 1, (1,))

            @pl.when(k == 1)
            def _():
                q_copy.wait_recv()
                for h in range(4):
                    qbd[g_far + h] = block_diagonal(qin[h])

        way = lax.rem(r + 1, 2)
        far = lax.rem(z + NZ + jnp.where(way == 0, 1 - k, k - 1), NZ)

        @pl.when((r >= 1) & ((way == 0) | (k > 1)))
        def _():
            compute(far * 2 + (r - 1) // 2)

        return carry

    share(0, (0,))
    lax.fori_loop(0, 20, tick, 0)
    share(4, (0,))
    shared(4, (0,))

    def last(yy, carry):
        compute(slab(4, 0) * 2 + yy)
        return carry

    lax.fori_loop(0, 2, last, 0)

    def finish(group, att_out, lse_out):
        for h in range(4):
            acc = acc_ref[group + h]
            m = m_ref[group + h]
            total = acc[HALF:HALF + 1]
            lse = m + jnp.log(total)
            lse_out[0, h:h + 1, :] = lse[:, :HALF]
            lse_out[1, h:h + 1, :] = lse[:, HALF:]
            ratio = acc[:HALF] / total
            out = ratio[:, :HALF] - lam_ref[h:h + 1, :] * ratio[:, HALF:]
            scale = lax.rsqrt(jnp.mean(out * out, axis=0, keepdims=True) + NORM_EPS)
            normed = out * scale * gain_ref[...]
            att_out[:, h * HALF:(h + 1) * HALF] = normed.T.astype(jnp.bfloat16)

    finish(g_far, attx, lsex)
    finish(g_own, att_ref.at[0], lse_ref.at[0])
    back = (remote(attx, attr, o_s.at[0], o_r.at[0], partner),
            remote(lsex, lser, o_s.at[1], o_r.at[1], partner))
    for copy in back:
        copy.start()

    q_copy.wait_send()
    for d in range(3):
        v_to_y(d).wait_send()
        k_to_y(0, 0, d).wait_send()
    to_sibling(0, 0, c).wait_send()

    def drain(k, carry):
        for way in (0, 1):
            for r in range(5):
                z_msg(k, r, way, 0).wait_send()
            for d in range(3):
                k_to_y(k, way, d).wait_send()
            to_sibling(k, way, c).wait_send()
        return carry

    lax.fori_loop(1, 4, drain, 0)
    for r in range(5):
        z_msg(4, r, 0 if r <= 2 else 1, 0).wait_send()
    for d in range(3):
        k_to_y(4, 0, d).wait_send()
    to_sibling(4, 0, c).wait_send()
    for copy in back:
        copy.wait()
    att_ref[1] = attr[...]
    lse_ref[1] = lser[...]


def attend(queries, keys_own, values_own, lam, head_gain):
    qt = jnp.transpose(queries * jnp.asarray(0.125, jnp.bfloat16), (1, 2, 0))
    vt = values_own.reshape(2, HALF, 128).transpose(0, 2, 1).reshape(ROWS, 128)
    bf, f32 = jnp.bfloat16, jnp.float32
    dma = pltpu.SemaphoreType.DMA
    vmem = pl.BlockSpec(memory_space=pltpu.VMEM)
    return pl.pallas_call(
        attention_kernel,
        out_shape=(
            jax.ShapeDtypeStruct((2, HALF, 512), bf),
            jax.ShapeDtypeStruct((2, 2, 4, HALF), f32),
        ),
        in_specs=[vmem] * 6,
        out_specs=(vmem, vmem),
        scratch_shapes=[
            pltpu.VMEM((NZ, NC, 2, NY, ROWS, 128), bf),
            pltpu.VMEM((8, 128, 256), bf),
            pltpu.VMEM((4, 128, 128), bf),
            pltpu.VMEM((8, 1, 256), f32),
            pltpu.VMEM((8, 144, 256), f32),
            pltpu.VMEM((HALF, 512), bf),
            pltpu.VMEM((2, 4, HALF), f32),
            pltpu.VMEM((HALF, 512), bf),
            pltpu.VMEM((2, 4, HALF), f32),
            *[pltpu.VMEM((KB, 256), f32)] * NB,
            *[pltpu.VMEM((KB, 256), bf)] * NB,
            *[pltpu.VMEM((1, 256), f32)] * NB,
            dma((2,)),
            dma((2, 5, 3)), dma((2, 5, 3)), dma((3,)), dma((3,)),
            dma((2, 5, 5)), dma((2, 5, 5)), dma((2, 5)), dma((2, 5)),
            dma, dma, dma((2,)), dma((2,)),
        ],
        compiler_params=pltpu.CompilerParams(
            collective_id=0, has_side_effects=True, vmem_limit_bytes=48 * 2**20
        ),
        name="attend",
    )(
        qt[:, :, :HALF], qt[:, :, HALF:], keys_own, vt,
        jnp.broadcast_to(lam[:, None], (4, HALF)),
        jnp.broadcast_to(head_gain[:, None], (128, HALF)),
    )


def local(
    tokens,
    norm_gain,
    query_weight,
    key_weight,
    value_weight,
    mix_lambda,
    head_gain,
    pool_weight,
    pool_mix,
    pool_scale,
    gate_weight,
    out_weight,
):
    model_width = tokens.shape[1]
    heads_local = query_weight.shape[1]
    group_width = pool_weight.shape[2]
    channels = gate_weight.shape[2]
    matrices = (
        query_weight.reshape(model_width, -1),
        key_weight.reshape(model_width, -1),
        value_weight.reshape(model_width, -1),
        pool_weight.reshape(model_width, -1),
        gate_weight.reshape(model_width, -1),
    )
    rows = copy_for_each(tokens, "tp").reshape(-1, model_width)
    inputs = rows.astype(jnp.float32)
    normed = (
        inputs
        * lax.rsqrt(jnp.mean(inputs * inputs, axis=1, keepdims=True) + NORM_EPS)
        * norm_gain
    ).astype(jnp.bfloat16)
    queries, keys_own, values_own, pool_in, gate_pre = [
        jnp.dot(normed, matrix, preferred_element_type=jnp.float32).astype(jnp.bfloat16)
        for matrix in matrices
    ]
    tok_rows = rows.shape[0]
    rim_prev = shifted(pool_in[tok_rows - WINDOW :], "sp", 1)
    att, lse = attend(
        queries.reshape(tok_rows, heads_local, 128), keys_own, values_own, mix_lambda, head_gain
    )
    attended = att.reshape(tok_rows, 512).astype(jnp.float32)
    log_out = jnp.concatenate([lse[0], lse[1]], axis=2)
    gate_pre = gate_pre.reshape(tok_rows, 2, channels)
    positions = lax.axis_index("sp") * tok_rows + jnp.arange(tok_rows, dtype=jnp.int32)
    extended = jnp.concatenate([rim_prev, pool_in], axis=0).astype(jnp.float32)
    window_span = jnp.left_shift(jnp.int32(2), lax.axis_index("tp"))
    window_sum = jnp.zeros((tok_rows, group_width), jnp.float32)
    for back_rows in range(WINDOW):
        window_sum = window_sum + jnp.where(
            back_rows < window_span,
            extended[WINDOW - back_rows : WINDOW - back_rows + tok_rows],
            0.0,
        )
    counts = jnp.minimum(positions + 1, window_span).astype(jnp.float32)
    means = window_sum / counts[:, None]
    pooled = (means - pool_in.astype(jnp.float32)).astype(jnp.bfloat16)
    group_parts = jnp.dot(pooled, pool_mix[0], preferred_element_type=jnp.float32) * pool_scale[0]
    merged = (
        jax.nn.sigmoid(gate_pre[:, 0].astype(jnp.float32)) * attended
        + jax.nn.sigmoid(gate_pre[:, 1].astype(jnp.float32)) * group_parts
    ).astype(jnp.bfloat16)
    mixed = sent_and_summed(
        jnp.dot(merged, out_weight, preferred_element_type=jnp.float32).astype(jnp.bfloat16),
        "tp",
    )
    return (mixed.astype(jnp.bfloat16), log_out)


def solution(mesh):
    in_specs = (
        P(("sp", "tp"), None),
        P(),
        P(None, "tp", None),
        P(None, "tp", None),
        P(None, "tp", None),
        P("tp"),
        P(),
        P(None, "tp", None),
        P("tp", None, None),
        P("tp", None),
        P(None, None, "tp"),
        P("tp", None),
    )
    out_specs = (P(("sp", "tp"), None), P(None, "tp", "sp"))
    return jax.shard_map(local, mesh=mesh, in_specs=in_specs, out_specs=out_specs, check_vma=False)
```

```python
import functools

import jax
import jax.numpy as jnp
from jax import lax
from jax.experimental import pallas as pl
from jax.experimental.pallas import tpu as pltpu
from jax.sharding import PartitionSpec as P

WINDOW = 16
NORM_EPS = 1e-06
MESH = pl.DeviceIdType.MESH
NEG = -1e30
NZ, NY, NC = 8, 4, 2
LAG, NB = 3, 4
ROWS = 256
HALF = 128
KB = 1024


def copy_for_each(array, axis):
    size = lax.axis_size(axis)
    return lax.all_to_all(
        jnp.broadcast_to(array[None], (size, *array.shape)), axis, 0, 0, tiled=True
    )


def project_kernel(
    tok_ref, gain_ref, wq, wk, wv, wp, wg,
    q_own, q_far, k_ref, vt_ref, pool_ref, rim_ref, gate_ref,
    normed, vq, vk, vv, vp, vg, sems,
):
    copies = [
        pltpu.make_async_copy(src, dst, sems.at[n])
        for n, (src, dst) in enumerate(((wk, vk), (wv, vv), (wq, vq), (wp, vp), (wg, vg)))
    ]
    for copy in copies:
        copy.start()
    gain = gain_ref[...]
    for b in range(0, ROWS, 32):
        x = tok_ref[b:b + 32, :].astype(jnp.float32)
        scale = lax.rsqrt(jnp.mean(x * x, axis=1, keepdims=True) + NORM_EPS)
        normed[b:b + 32, :] = (x * scale * gain).astype(jnp.bfloat16)

    def project(weight):
        return jnp.dot(normed[...], weight, preferred_element_type=jnp.float32)

    copies[0].wait()
    k_ref[...] = project(vk[...]).astype(jnp.bfloat16)
    copies[1].wait()
    v = project(vv[...])
    for b in (0, HALF):
        vt_ref[b:b + HALF, :] = v[b:b + HALF].T.astype(jnp.bfloat16)
    copies[2].wait()
    for h in range(4):
        q = project(vq[:, h * 128:(h + 1) * 128]) * 0.125
        q_own[h] = q[:HALF].T.astype(jnp.bfloat16)
        q_far[h] = q[HALF:].T.astype(jnp.bfloat16)
    copies[3].wait()
    pool_in = project(vp[...]).astype(jnp.bfloat16)
    pool_ref[...] = pool_in
    rim_ref[...] = pool_in[ROWS - WINDOW:]
    copies[4].wait()
    for g in (0, 1):
        gate_ref[g] = project(vg[g]).astype(jnp.bfloat16)


def project(rows, norm_gain, wq, wk, wv, wp, wg):
    bf = jnp.bfloat16
    vmem = pl.BlockSpec(memory_space=pltpu.VMEM)
    anywhere = pl.BlockSpec(memory_space=pl.ANY)
    shape = jax.ShapeDtypeStruct
    return pl.pallas_call(
        project_kernel,
        out_shape=(
            shape((4, 128, HALF), bf), shape((4, 128, HALF), bf),
            shape((ROWS, 128), bf), shape((ROWS, 128), bf),
            shape((ROWS, 512), bf), shape((WINDOW, 512), bf), shape((2, ROWS, 512), bf),
        ),
        in_specs=[vmem, vmem] + [anywhere] * 5,
        out_specs=(vmem,) * 7,
        scratch_shapes=[
            pltpu.VMEM((ROWS, 2048), bf),
            pltpu.VMEM(wq.shape, bf), pltpu.VMEM(wk.shape, bf), pltpu.VMEM(wv.shape, bf),
            pltpu.VMEM(wp.shape, bf), pltpu.VMEM(wg.shape, bf),
            pltpu.SemaphoreType.DMA((5,)),
        ],
        compiler_params=pltpu.CompilerParams(vmem_limit_bytes=48 * 2**20),
        cost_estimate=pl.CostEstimate(
            flops=2 * ROWS * 2048 * 2304, bytes_accessed=10**7, transcendentals=0
        ),
        name="project",
    )(rows, norm_gain[None], wq, wk, wv, wp, wg)


def output_kernel(
    att_ref, gate_ref, pool_ref, rim_ref, mix_ref, scale_ref, weight_ref,
    out_ref,
    merged, part, got, s_sem, r_sem,
):
    x = lax.axis_index("tp")
    peers = [{"tp": lax.rem(x + d, 4)} for d in (1, 2, 3)]
    barrier = pltpu.get_barrier_semaphore()
    for peer in peers:
        pl.semaphore_signal(barrier, inc=1, device_id=peer, device_id_type=MESH)

    f32, bf = jnp.float32, jnp.bfloat16
    for cb in range(0, 512, 128):
        cols = slice(cb, cb + 128)
        own = pool_ref[:, cols].astype(f32)
        rim = jnp.where(lax.axis_index("sp") == 0, 0.0, rim_ref[:, cols].astype(f32))
        sums = jnp.concatenate([rim, own], axis=0)
        picked = sums
        for n, shift in enumerate((1, 2, 4, 8)):
            sums = sums + pltpu.roll(sums, shift, 0)
            picked = jnp.where(x >= n, sums, picked)
        position = lax.axis_index("sp") * ROWS + lax.broadcasted_iota(jnp.int32, (ROWS, 128), 0)
        span = jnp.left_shift(jnp.int32(2), x)
        counts = jnp.minimum(position + 1, span).astype(f32)
        merged[:, cols] = (picked[WINDOW:] / counts - own).astype(bf)
    pool_out = jnp.dot(merged[...], mix_ref[...], preferred_element_type=f32) * scale_ref[...]
    attended = jnp.concatenate([att_ref[0], att_ref[1]], axis=0).astype(f32)
    merged[...] = (
        jax.nn.sigmoid(gate_ref[0].astype(f32)) * attended
        + jax.nn.sigmoid(gate_ref[1].astype(f32)) * pool_out
    ).astype(bf)

    def partial(d):
        first = pl.multiple_of(lax.rem(x + d, 4) * 64, 64)
        return jnp.dot(merged[pl.ds(first, 64), :], weight_ref[...], preferred_element_type=f32)

    def send(d):
        return pltpu.make_async_remote_copy(
            src_ref=part.at[d - 1], dst_ref=got.at[d - 1],
            send_sem=s_sem.at[d - 1], recv_sem=r_sem.at[d - 1],
            device_id=peers[d - 1], device_id_type=MESH,
        )

    part[1] = partial(2).astype(bf)
    pl.semaphore_wait(barrier, 3)
    part[0] = partial(1).astype(bf)
    send(2).start()
    part[2] = partial(3).astype(bf)
    send(1).start()
    total = partial(0).astype(bf).astype(f32)
    send(3).start()
    for d in (1, 3, 2):
        send(d).wait()
        total = total + got[d - 1].astype(f32)
    out_ref[...] = total.astype(bf)


def output(att, gates, pool_in, rim, mix, scale, weight):
    bf = jnp.bfloat16
    vmem = pl.BlockSpec(memory_space=pltpu.VMEM)
    dma = pltpu.SemaphoreType.DMA
    return pl.pallas_call(
        output_kernel,
        out_shape=jax.ShapeDtypeStruct((64, 2048), bf),
        in_specs=[vmem] * 7,
        out_specs=vmem,
        scratch_shapes=[
            pltpu.VMEM((ROWS, 512), bf),
            pltpu.VMEM((3, 64, 2048), bf),
            pltpu.VMEM((3, 64, 2048), bf),
            dma((3,)), dma((3,)),
        ],
        compiler_params=pltpu.CompilerParams(
            collective_id=1, has_side_effects=True, vmem_limit_bytes=32 * 2**20
        ),
        name="output",
    )(att, gates, pool_in, rim, mix, scale, weight)


def attention_kernel(
    q_ref, qs_ref, k_ref, v_ref, rim_ref, lam_ref, gain_ref,
    att_ref, lse_ref, rim_out,
    kv, qbd, qin, m_ref, acc_ref, attx, lsex, attr, lser, rim_in,
    *rest,
):
    sb, pb, bm = rest[:NB], rest[NB:2 * NB], rest[2 * NB:3 * NB]
    (own_sem, y_s, y_r, vy_s, vy_r, z_s, z_r,
     sib_s, sib_r, q_s, q_r, o_s, o_r, rim_s, rim_r) = rest[3 * NB:]
    me = lax.axis_index("sp")
    z, y, c = me // (NY * NC), (me // NC) % NY, me % NC

    def at(zz, yy, cc):
        return {"sp": (zz * NY + yy) * NC + cc}

    sibling = at(z, y, 1 - c)
    partner = at(NZ - 1 - z, NY - 1 - y, c)
    z_next = [at((z + 1) % NZ, y, c), at((z + NZ - 1) % NZ, y, c)]
    y_peers = [at(z, (y + d) % NY, c) for d in (1, 2, 3)]

    barrier = pltpu.get_barrier_semaphore()
    n_sp = NZ * NY * NC
    after, before = {"sp": lax.rem(me + 1, n_sp)}, {"sp": lax.rem(me + n_sp - 1, n_sp)}
    peers = [sibling, partner, *z_next, *y_peers, after, before]
    for peer in peers:
        pl.semaphore_signal(barrier, inc=1, device_id=peer, device_id_type=MESH)
    pl.semaphore_wait(barrier, len(peers))

    def remote(src, dst, s, r, dev):
        return pltpu.make_async_remote_copy(
            src_ref=src, dst_ref=dst, send_sem=s, recv_sem=r,
            device_id=dev, device_id_type=MESH,
        )

    def slab(k, way):
        return lax.rem(z + NZ + (k if way else -k), NZ)

    def k_to_y(k, way, d):
        piece = kv.at[slab(k, way), c, 0, y]
        return remote(piece, piece, y_s.at[way, k, d], y_r.at[way, k, d], y_peers[d])

    def k_from_y(k, way, d):
        piece = kv.at[slab(k, way), c, 0, lax.rem(y + NY - (d + 1), NY)]
        return remote(piece, piece, y_s.at[way, k, d], y_r.at[way, k, d], y_peers[d])

    def v_to_y(d):
        return remote(v_ref, kv.at[z, c, 1, y], vy_s.at[d], vy_r.at[d], y_peers[d])

    def v_from_y(d):
        yy = lax.rem(y + NY - (d + 1), NY)
        return remote(v_ref, kv.at[z, c, 1, yy], vy_s.at[d], vy_r.at[d], y_peers[d])

    def z_piece(zs, r):
        kind = jnp.minimum(r, 1)
        return kv.at[zs, c, kind, lax.rem(y + jnp.maximum(r - 1, 0), NY)]

    def z_msg(k, r, way, src_k, src=None):
        piece = z_piece(slab(src_k, way), r)
        return remote(
            piece if src is None else src, piece,
            z_s.at[way, k, r], z_r.at[way, k, r], z_next[way],
        )

    def to_sibling(k, way, cc):
        part = kv.at[slab(k, way), cc]
        return remote(part, part, sib_s.at[way, k], sib_r.at[way, k], sibling)

    own_k = pltpu.make_async_copy(k_ref, kv.at[z, c, 0, y], own_sem.at[0])
    own_v = pltpu.make_async_copy(v_ref, kv.at[z, c, 1, y], own_sem.at[1])
    own_k.start()
    own_v.start()
    for d in (0, 2, 1):
        v_to_y(d).start()
    for way in (0, 1):
        z_msg(1, 0, way, 0, k_ref).start()
        z_msg(1, 1, way, 0, v_ref).start()
    q_copy = remote(qs_ref, qin, q_s, q_r, partner)
    q_copy.start()
    rim_copy = remote(rim_ref, rim_in, rim_s, rim_r, after)
    rim_copy.start()
    own_k.wait()
    for d in (0, 2, 1):
        k_to_y(0, 0, d).start()
    own_v.wait()

    m_ref[...] = jnp.full_like(m_ref, NEG)
    acc_ref[...] = jnp.zeros_like(acc_ref)
    is_low = z < NZ // 2
    g_own = jnp.where(is_low, 0, 4)
    g_far = 4 - g_own

    def block_diagonal(q):
        top = lax.broadcasted_iota(jnp.int32, (HALF, HALF), 0) < 64
        zero = jnp.zeros_like(q)
        return jnp.concatenate([jnp.where(top, q, zero), jnp.where(top, zero, q)], axis=1)

    for h in range(4):
        qbd[g_own + h] = block_diagonal(q_ref[h])

    for r in (2, 4, 3):
        v_from_y(NY - r).wait_recv()
        for way in (0, 1):
            z_msg(1, r, way, 0).start()

    mine = (z * NY + y) // 2
    lo = jnp.minimum(mine, 15 - mine)
    hi = 15 - lo

    ones = jnp.ones((16, KB), jnp.bfloat16)

    def pieces(i, kind):
        zs, yy = i // 2, 2 * lax.rem(i, 2)
        return [kv[zs, cc, kind, yy + d] for d in (0, 1) for cc in (0, 1)]

    def keys(i):
        return jnp.concatenate(pieces(i, 0), axis=0)

    def values(i):
        halves = [v[a:a + HALF] for v in pieces(i, 1) for a in (0, HALF)]
        return jnp.concatenate([jnp.concatenate(halves, axis=1), ones], axis=0)

    def scores(i, t, slot, base=None):
        s = jnp.dot(keys(i), qbd[t], preferred_element_type=jnp.float32)
        if base is not None:
            key_pos = i * KB + lax.broadcasted_iota(jnp.int32, (KB, 2 * HALF), 0)
            row = lax.broadcasted_iota(jnp.int32, (KB, 2 * HALF), 1)
            row_pos = base + jnp.where(row < HALF, row, row - HALF)
            s = jnp.where(key_pos <= row_pos, s, NEG)
        sb[slot][...] = s
        bm[slot][...] = jnp.max(s, axis=0, keepdims=True)

    def weigh(i, t, slot):
        old = m_ref[t]
        new = jnp.maximum(old, bm[slot][...])
        m_ref[t] = new
        pb[slot][...] = jnp.exp(sb[slot][...] - new).astype(jnp.bfloat16)
        acc_ref[t] = acc_ref[t] * jnp.exp(old - new) + jnp.dot(
            values(i), pb[slot][...], preferred_element_type=jnp.float32
        )

    def block(items, base=None):
        n = len(items)
        for u in range(LAG):
            scores(*items[u], u % NB, base)
        for u in range(n):
            if u + LAG < n:
                scores(*items[u + LAG], (u + LAG) % NB, base)
            weigh(*items[u], u % NB)

    p_own = me * ROWS
    p_far = partner["sp"] * ROWS + HALF
    base_lo = jnp.where(is_low, p_own, p_far)
    base_hi = jnp.where(is_low, p_far, p_own)

    def compute(zs, half):
        i = 2 * zs + half
        whole = (2 * zs >= lo) & (2 * zs + 1 < hi)

        @pl.when(i < lo)
        def _():
            block([(i, t) for t in range(8)])

        @pl.when(whole & (half == 1))
        def _():
            block([(2 * zs + w, 4 + u) for w in (0, 1) for u in range(4)])

        @pl.when((i >= lo) & (i < hi) & jnp.logical_not(whole))
        def _():
            block([(i, 4 + u) for u in range(4)])

        @pl.when((i == lo) | (i == hi))
        def _():
            first = jnp.where(i == lo, 0, 4)
            block([(i, first + u) for u in range(4)], jnp.where(i == lo, base_lo, base_hi))

    def share(k, ways):
        for way in ways:
            for d in range(3):
                k_from_y(k, way, d).wait_recv()
            to_sibling(k, way, c).start()

    def shared(k, ways):
        for way in ways:
            to_sibling(k, way, 1 - c).wait_recv()

    def serve(k, r, way, forward):
        z_msg(k, r, way, k).wait_recv()
        if forward is not None:
            @pl.when(forward)
            def _():
                z_msg(k + 1, r, way, k).start()

        @pl.when(r == 0)
        def _():
            for d in (0, 2, 1):
                k_to_y(k, way, d).start()

    def both(k, r):
        serve(k, r, 0, (k < 3) | (r <= 2))
        serve(k, r, 1, (k < 3) | (r >= 3))

    def tick(n, carry):
        k, r = n // 5 + 1, lax.rem(n, 5)

        @pl.when(k <= 3)
        def _():
            both(k, r)

        @pl.when((k == 4) & (r <= 2))
        def _():
            serve(k, r, 0, None)

        @pl.when((k == 4) & (r <= 1))
        def _():
            z_msg(k, r + 3, 1, k).wait_recv()

        @pl.when((r == 4) & (k <= 3))
        def _():
            share(k, (0, 1))

        @pl.when(r == 1)
        def _():
            shared(k - 1, (0,))

            @pl.when(k > 1)
            def _():
                shared(k - 1, (1,))

            @pl.when(k == 1)
            def _():
                q_copy.wait_recv()
                for h in range(4):
                    qbd[g_far + h] = block_diagonal(qin[h])

        way = lax.rem(r + 1, 2)
        far = lax.rem(z + NZ + jnp.where(way == 0, 1 - k, k - 1), NZ)

        @pl.when((r >= 1) & ((way == 0) | (k > 1)))
        def _():
            compute(far, (r - 1) // 2)

        return carry

    share(0, (0,))
    lax.fori_loop(0, 20, tick, 0)
    share(4, (0,))
    shared(4, (0,))

    def last(yy, carry):
        compute(slab(4, 0), yy)
        return carry

    lax.fori_loop(0, 2, last, 0)

    def finish(group, att_out, lse_out):
        for h in range(4):
            acc = acc_ref[group + h]
            m = m_ref[group + h]
            total = acc[HALF:HALF + 1]
            lse = m + jnp.log(total)
            lse_out[0, h:h + 1, :] = lse[:, :HALF]
            lse_out[1, h:h + 1, :] = lse[:, HALF:]
            ratio = acc[:HALF] / total
            out = ratio[:, :HALF] - lam_ref[h:h + 1, :] * ratio[:, HALF:]
            scale = lax.rsqrt(jnp.mean(out * out, axis=0, keepdims=True) + NORM_EPS)
            normed = out * scale * gain_ref[...]
            att_out[:, h * HALF:(h + 1) * HALF] = normed.T.astype(jnp.bfloat16)

    finish(g_far, attx, lsex)
    finish(g_own, att_ref.at[0], lse_ref.at[0])
    back = (remote(attx, attr, o_s.at[0], o_r.at[0], partner),
            remote(lsex, lser, o_s.at[1], o_r.at[1], partner))
    for copy in back:
        copy.start()

    q_copy.wait_send()
    rim_copy.wait()
    rim_out[...] = rim_in[...]
    for d in range(3):
        v_to_y(d).wait_send()
        k_to_y(0, 0, d).wait_send()
    to_sibling(0, 0, c).wait_send()

    def drain(k, carry):
        for way in (0, 1):
            for r in range(5):
                z_msg(k, r, way, 0).wait_send()
            for d in range(3):
                k_to_y(k, way, d).wait_send()
            to_sibling(k, way, c).wait_send()
        return carry

    lax.fori_loop(1, 4, drain, 0)
    for r in range(5):
        z_msg(4, r, 0 if r <= 2 else 1, 0).wait_send()
    for d in range(3):
        k_to_y(4, 0, d).wait_send()
    to_sibling(4, 0, c).wait_send()
    for copy in back:
        copy.wait()
    att_ref[1] = attr[...]
    lse_ref[1] = lser[...]


def attend(q_own, q_far, keys_own, vt, rim_rows, lam, head_gain):
    bf, f32 = jnp.bfloat16, jnp.float32
    dma = pltpu.SemaphoreType.DMA
    vmem = pl.BlockSpec(memory_space=pltpu.VMEM)
    return pl.pallas_call(
        attention_kernel,
        out_shape=(
            jax.ShapeDtypeStruct((2, HALF, 512), bf),
            jax.ShapeDtypeStruct((2, 2, 4, HALF), f32),
            jax.ShapeDtypeStruct((WINDOW, 512), bf),
        ),
        in_specs=[vmem] * 7,
        out_specs=(vmem,) * 3,
        scratch_shapes=[
            pltpu.VMEM((NZ, NC, 2, NY, ROWS, 128), bf),
            pltpu.VMEM((8, 128, 256), bf),
            pltpu.VMEM((4, 128, 128), bf),
            pltpu.VMEM((8, 1, 256), f32),
            pltpu.VMEM((8, 144, 256), f32),
            pltpu.VMEM((HALF, 512), bf),
            pltpu.VMEM((2, 4, HALF), f32),
            pltpu.VMEM((HALF, 512), bf),
            pltpu.VMEM((2, 4, HALF), f32),
            pltpu.VMEM((WINDOW, 512), bf),
            *[pltpu.VMEM((KB, 256), f32)] * NB,
            *[pltpu.VMEM((KB, 256), bf)] * NB,
            *[pltpu.VMEM((1, 256), f32)] * NB,
            dma((2,)),
            dma((2, 5, 3)), dma((2, 5, 3)), dma((3,)), dma((3,)),
            dma((2, 5, 5)), dma((2, 5, 5)), dma((2, 5)), dma((2, 5)),
            dma, dma, dma((2,)), dma((2,)), dma, dma,
        ],
        compiler_params=pltpu.CompilerParams(
            collective_id=0, has_side_effects=True, vmem_limit_bytes=48 * 2**20
        ),
        cost_estimate=pl.CostEstimate(
            flops=2 * 10**10, bytes_accessed=10**6, transcendentals=2 * 10**7
        ),
        name="attend",
    )(
        q_own, q_far, keys_own, vt, rim_rows,
        jnp.broadcast_to(lam[:, None], (4, HALF)),
        jnp.broadcast_to(head_gain[:, None], (128, HALF)),
    )


def local(
    tokens,
    norm_gain,
    query_weight,
    key_weight,
    value_weight,
    mix_lambda,
    head_gain,
    pool_weight,
    pool_mix,
    pool_scale,
    gate_weight,
    out_weight,
):
    model_width = tokens.shape[1]
    rows = copy_for_each(tokens, "tp").reshape(-1, model_width)
    q_own, q_far, keys_own, vt, pool_in, rim_rows, gates = project(
        rows,
        norm_gain,
        query_weight.reshape(model_width, -1),
        key_weight.reshape(model_width, -1),
        value_weight.reshape(model_width, -1),
        pool_weight.reshape(model_width, -1),
        jnp.transpose(gate_weight, (1, 0, 2)),
    )
    att, lse, rim = attend(q_own, q_far, keys_own, vt, rim_rows, mix_lambda, head_gain)
    mixed = output(att, gates, pool_in, rim, pool_mix[0], pool_scale, out_weight)
    return (mixed, jnp.concatenate([lse[0], lse[1]], axis=2))


def solution(mesh):
    in_specs = (
        P(("sp", "tp"), None),
        P(),
        P(None, "tp", None),
        P(None, "tp", None),
        P(None, "tp", None),
        P("tp"),
        P(),
        P(None, "tp", None),
        P("tp", None, None),
        P("tp", None),
        P(None, None, "tp"),
        P("tp", None),
    )
    out_specs = (P(("sp", "tp"), None), P(None, "tp", "sp"))
    return jax.shard_map(local, mesh=mesh, in_specs=in_specs, out_specs=out_specs, check_vma=False)
```

```python
import functools

import jax
import jax.numpy as jnp
from jax import lax
from jax.experimental import pallas as pl
from jax.experimental.pallas import tpu as pltpu
from jax.sharding import PartitionSpec as P

WINDOW = 16
NORM_EPS = 1e-06
MESH = pl.DeviceIdType.MESH
NEG = -1e30
NZ, NY, NC = 8, 4, 2
LAG, NB = 3, 4
ROWS = 256
HALF = 128
KB = 1024


def copy_for_each(array, axis):
    size = lax.axis_size(axis)
    return lax.all_to_all(
        jnp.broadcast_to(array[None], (size, *array.shape)), axis, 0, 0, tiled=True
    )


def project_kernel(
    tok_ref, gain_ref, wq, wk, wv, wp, wg,
    q_own, q_far, k_ref, vt_ref, pool_ref, rim_ref, gate_ref,
    normed, vq, vk, vv, vp, vg, sems,
):
    copies = [
        pltpu.make_async_copy(src, dst, sems.at[n])
        for n, (src, dst) in enumerate(((wk, vk), (wv, vv), (wq, vq), (wp, vp), (wg, vg)))
    ]
    for copy in copies:
        copy.start()
    gain = gain_ref[...]
    for b in range(0, ROWS, 32):
        x = tok_ref[b:b + 32, :].astype(jnp.float32)
        scale = lax.rsqrt(jnp.mean(x * x, axis=1, keepdims=True) + NORM_EPS)
        normed[b:b + 32, :] = (x * scale * gain).astype(jnp.bfloat16)

    def project(weight):
        return jnp.dot(normed[...], weight, preferred_element_type=jnp.float32)

    copies[0].wait()
    k_ref[...] = project(vk[...]).astype(jnp.bfloat16)
    copies[1].wait()
    v = project(vv[...])
    for b in (0, HALF):
        vt_ref[b:b + HALF, :] = v[b:b + HALF].T.astype(jnp.bfloat16)
    copies[2].wait()
    for h in range(4):
        q = project(vq[:, h * 128:(h + 1) * 128]) * 0.125
        q_own[h] = q[:HALF].T.astype(jnp.bfloat16)
        q_far[h] = q[HALF:].T.astype(jnp.bfloat16)
    copies[3].wait()
    pool_in = project(vp[...]).astype(jnp.bfloat16)
    pool_ref[...] = pool_in
    rim_ref[...] = pool_in[ROWS - WINDOW:]
    copies[4].wait()
    for g in (0, 1):
        gate_ref[g] = project(vg[g]).astype(jnp.bfloat16)


def project(rows, norm_gain, wq, wk, wv, wp, wg):
    bf = jnp.bfloat16
    vmem = pl.BlockSpec(memory_space=pltpu.VMEM)
    anywhere = pl.BlockSpec(memory_space=pl.ANY)
    shape = jax.ShapeDtypeStruct
    return pl.pallas_call(
        project_kernel,
        out_shape=(
            shape((4, 128, HALF), bf), shape((4, 128, HALF), bf),
            shape((ROWS, 128), bf), shape((ROWS, 128), bf),
            shape((ROWS, 512), bf), shape((WINDOW, 512), bf), shape((2, ROWS, 512), bf),
        ),
        in_specs=[vmem, vmem] + [anywhere] * 5,
        out_specs=(vmem,) * 7,
        scratch_shapes=[
            pltpu.VMEM((ROWS, 2048), bf),
            pltpu.VMEM(wq.shape, bf), pltpu.VMEM(wk.shape, bf), pltpu.VMEM(wv.shape, bf),
            pltpu.VMEM(wp.shape, bf), pltpu.VMEM(wg.shape, bf),
            pltpu.SemaphoreType.DMA((5,)),
        ],
        compiler_params=pltpu.CompilerParams(vmem_limit_bytes=48 * 2**20),
        cost_estimate=pl.CostEstimate(
            flops=2 * ROWS * 2048 * 2304, bytes_accessed=10**7, transcendentals=0
        ),
        name="project",
    )(rows, norm_gain[None], wq, wk, wv, wp, wg)


def output_kernel(
    att_ref, gate_ref, pool_ref, rim_ref, mix_ref, scale_ref, weight_ref,
    out_ref,
    merged, part, got, s_sem, r_sem,
):
    x = lax.axis_index("tp")
    peers = [{"tp": lax.rem(x + d, 4)} for d in (1, 2, 3)]
    barrier = pltpu.get_barrier_semaphore()
    for peer in peers:
        pl.semaphore_signal(barrier, inc=1, device_id=peer, device_id_type=MESH)

    f32, bf = jnp.float32, jnp.bfloat16
    for cb in range(0, 512, 128):
        cols = slice(cb, cb + 128)
        own = pool_ref[:, cols].astype(f32)
        rim = jnp.where(lax.axis_index("sp") == 0, 0.0, rim_ref[:, cols].astype(f32))
        sums = jnp.concatenate([rim, own], axis=0)
        picked = sums
        for n, shift in enumerate((1, 2, 4, 8)):
            sums = sums + pltpu.roll(sums, shift, 0)
            picked = jnp.where(x >= n, sums, picked)
        position = lax.axis_index("sp") * ROWS + lax.broadcasted_iota(jnp.int32, (ROWS, 128), 0)
        span = jnp.left_shift(jnp.int32(2), x)
        counts = jnp.minimum(position + 1, span).astype(f32)
        merged[:, cols] = (picked[WINDOW:] / counts - own).astype(bf)
    pool_out = jnp.dot(merged[...], mix_ref[...], preferred_element_type=f32) * scale_ref[...]
    attended = jnp.concatenate([att_ref[0], att_ref[1]], axis=0).astype(f32)
    merged[...] = (
        jax.nn.sigmoid(gate_ref[0].astype(f32)) * attended
        + jax.nn.sigmoid(gate_ref[1].astype(f32)) * pool_out
    ).astype(bf)

    def partial(d):
        first = pl.multiple_of(lax.rem(x + d, 4) * 64, 64)
        return jnp.dot(merged[pl.ds(first, 64), :], weight_ref[...], preferred_element_type=f32)

    def send(d):
        return pltpu.make_async_remote_copy(
            src_ref=part.at[d - 1], dst_ref=got.at[d - 1],
            send_sem=s_sem.at[d - 1], recv_sem=r_sem.at[d - 1],
            device_id=peers[d - 1], device_id_type=MESH,
        )

    part[1] = partial(2).astype(bf)
    pl.semaphore_wait(barrier, 3)
    part[0] = partial(1).astype(bf)
    send(2).start()
    part[2] = partial(3).astype(bf)
    send(1).start()
    total = partial(0).astype(bf).astype(f32)
    send(3).start()
    for d in (1, 3, 2):
        send(d).wait()
        total = total + got[d - 1].astype(f32)
    out_ref[...] = total.astype(bf)


def output(att, gates, pool_in, rim, mix, scale, weight):
    bf = jnp.bfloat16
    vmem = pl.BlockSpec(memory_space=pltpu.VMEM)
    dma = pltpu.SemaphoreType.DMA
    return pl.pallas_call(
        output_kernel,
        out_shape=jax.ShapeDtypeStruct((64, 2048), bf),
        in_specs=[vmem] * 7,
        out_specs=vmem,
        scratch_shapes=[
            pltpu.VMEM((ROWS, 512), bf),
            pltpu.VMEM((3, 64, 2048), bf),
            pltpu.VMEM((3, 64, 2048), bf),
            dma((3,)), dma((3,)),
        ],
        compiler_params=pltpu.CompilerParams(
            collective_id=1, has_side_effects=True, vmem_limit_bytes=32 * 2**20
        ),
        name="output",
    )(att, gates, pool_in, rim, mix, scale, weight)


def attention_kernel(
    q_ref, qs_ref, k_ref, v_ref, rim_ref, lam_ref, gain_ref,
    att_ref, lse_ref, rim_out,
    kv, qbd, m_ref, acc_ref, rim_in,
    *rest,
):
    sb, pb, bm = rest[:NB], rest[NB:2 * NB], rest[2 * NB:3 * NB]
    (own_sem, y_s, y_r, vy_s, vy_r, z_s, z_r,
     sib_s, sib_r, rim_s, rim_r) = rest[3 * NB:]
    me = lax.axis_index("sp")
    z, y, c = me // (NY * NC), (me // NC) % NY, me % NC

    def at(zz, yy, cc):
        return {"sp": (zz * NY + yy) * NC + cc}

    sibling = at(z, y, 1 - c)
    z_next = [at((z + 1) % NZ, y, c), at((z + NZ - 1) % NZ, y, c)]
    y_peers = [at(z, (y + d) % NY, c) for d in (1, 2, 3)]

    barrier = pltpu.get_barrier_semaphore()
    n_sp = NZ * NY * NC
    after, before = {"sp": lax.rem(me + 1, n_sp)}, {"sp": lax.rem(me + n_sp - 1, n_sp)}
    peers = [sibling, *z_next, *y_peers, after, before]
    for peer in peers:
        pl.semaphore_signal(barrier, inc=1, device_id=peer, device_id_type=MESH)
    pl.semaphore_wait(barrier, len(peers))

    def remote(src, dst, s, r, dev):
        return pltpu.make_async_remote_copy(
            src_ref=src, dst_ref=dst, send_sem=s, recv_sem=r,
            device_id=dev, device_id_type=MESH,
        )

    def slab(k, way):
        return lax.rem(z + NZ + (k if way else -k), NZ)

    def k_to_y(k, way, d):
        piece = kv.at[slab(k, way), c, 0, y]
        return remote(piece, piece, y_s.at[way, k, d], y_r.at[way, k, d], y_peers[d])

    def k_from_y(k, way, d):
        piece = kv.at[slab(k, way), c, 0, lax.rem(y + NY - (d + 1), NY)]
        return remote(piece, piece, y_s.at[way, k, d], y_r.at[way, k, d], y_peers[d])

    def v_to_y(d):
        return remote(v_ref, kv.at[z, c, 1, y], vy_s.at[d], vy_r.at[d], y_peers[d])

    def v_from_y(d):
        yy = lax.rem(y + NY - (d + 1), NY)
        return remote(v_ref, kv.at[z, c, 1, yy], vy_s.at[d], vy_r.at[d], y_peers[d])

    def z_piece(zs, r):
        kind = jnp.minimum(r, 1)
        return kv.at[zs, c, kind, lax.rem(y + jnp.maximum(r - 1, 0), NY)]

    def z_msg(k, r, way, src_k, src=None):
        piece = z_piece(slab(src_k, way), r)
        return remote(
            piece if src is None else src, piece,
            z_s.at[way, k, r], z_r.at[way, k, r], z_next[way],
        )

    def to_sibling(k, way, cc):
        part = kv.at[slab(k, way), cc]
        return remote(part, part, sib_s.at[way, k], sib_r.at[way, k], sibling)

    own_k = pltpu.make_async_copy(k_ref, kv.at[z, c, 0, y], own_sem.at[0])
    own_v = pltpu.make_async_copy(v_ref, kv.at[z, c, 1, y], own_sem.at[1])
    own_k.start()
    own_v.start()
    for d in (0, 2, 1):
        v_to_y(d).start()
    for way in (0, 1):
        z_msg(1, 0, way, 0, k_ref).start()
        z_msg(1, 1, way, 0, v_ref).start()
    rim_copy = remote(rim_ref, rim_in, rim_s, rim_r, after)
    rim_copy.start()
    own_k.wait()
    for d in (0, 2, 1):
        k_to_y(0, 0, d).start()
    own_v.wait()

    m_ref[...] = jnp.full_like(m_ref, NEG)
    acc_ref[...] = jnp.zeros_like(acc_ref)

    def block_diagonal(q):
        top = lax.broadcasted_iota(jnp.int32, (HALF, HALF), 0) < 64
        zero = jnp.zeros_like(q)
        return jnp.concatenate([jnp.where(top, q, zero), jnp.where(top, zero, q)], axis=1)

    for h in range(4):
        qbd[h] = block_diagonal(q_ref[h])
        qbd[4 + h] = block_diagonal(qs_ref[h])

    for r in (2, 4, 3):
        v_from_y(NY - r).wait_recv()
        for way in (0, 1):
            z_msg(1, r, way, 0).start()

    mine = (z * NY + y) // 2

    ones = jnp.ones((16, KB), jnp.bfloat16)

    def pieces(i, kind):
        zs, yy = i // 2, 2 * lax.rem(i, 2)
        return [kv[zs, cc, kind, yy + d] for d in (0, 1) for cc in (0, 1)]

    def keys(i):
        return jnp.concatenate(pieces(i, 0), axis=0)

    def values(i):
        halves = [v[a:a + HALF] for v in pieces(i, 1) for a in (0, HALF)]
        return jnp.concatenate([jnp.concatenate(halves, axis=1), ones], axis=0)

    def scores(i, t, slot, masked=False):
        s = jnp.dot(keys(i), qbd[t], preferred_element_type=jnp.float32)
        if masked:
            base = me * ROWS + t // 4 * HALF
            key_pos = i * KB + lax.broadcasted_iota(jnp.int32, (KB, 2 * HALF), 0)
            row = lax.broadcasted_iota(jnp.int32, (KB, 2 * HALF), 1)
            row_pos = base + jnp.where(row < HALF, row, row - HALF)
            s = jnp.where(key_pos <= row_pos, s, NEG)
        sb[slot][...] = s
        bm[slot][...] = jnp.max(s, axis=0, keepdims=True)

    def weigh(i, t, slot):
        old = m_ref[t]
        new = jnp.maximum(old, bm[slot][...])
        m_ref[t] = new
        pb[slot][...] = jnp.exp(sb[slot][...] - new).astype(jnp.bfloat16)
        acc_ref[t] = acc_ref[t] * jnp.exp(old - new) + jnp.dot(
            values(i), pb[slot][...], preferred_element_type=jnp.float32
        )

    def block(items, masked=False):
        n = len(items)
        for u in range(LAG):
            scores(*items[u], u % NB, masked)
        for u in range(n):
            if u + LAG < n:
                scores(*items[u + LAG], (u + LAG) % NB, masked)
            weigh(*items[u], u % NB)

    def compute(zs, half):
        first = 2 * zs
        i = first + half
        whole = first + 1 < mine

        @pl.when(whole & (half == 1))
        def _():
            block([(first + w, t) for w in (0, 1) for t in range(8)])

        @pl.when((i < mine) & jnp.logical_not(whole))
        def _():
            block([(i, t) for t in range(8)])

        @pl.when(i == mine)
        def _():
            block([(i, t) for t in range(8)], True)

    def share(k, ways):
        for way in ways:
            for d in range(3):
                k_from_y(k, way, d).wait_recv()
            to_sibling(k, way, c).start()

    def shared(k, ways):
        for way in ways:
            to_sibling(k, way, 1 - c).wait_recv()

    def serve(k, r, way, forward):
        z_msg(k, r, way, k).wait_recv()
        if forward is not None:
            @pl.when(forward)
            def _():
                z_msg(k + 1, r, way, k).start()

        @pl.when(r == 0)
        def _():
            for d in (0, 2, 1):
                k_to_y(k, way, d).start()

    def both(k, r):
        serve(k, r, 0, (k < 3) | (r <= 2))
        serve(k, r, 1, (k < 3) | (r >= 3))

    def tick(n, carry):
        k, r = n // 5 + 1, lax.rem(n, 5)

        @pl.when(k <= 3)
        def _():
            both(k, r)

        @pl.when((k == 4) & (r <= 2))
        def _():
            serve(k, r, 0, None)

        @pl.when((k == 4) & (r <= 1))
        def _():
            z_msg(k, r + 3, 1, k).wait_recv()

        @pl.when((r == 4) & (k <= 3))
        def _():
            share(k, (0, 1))

        @pl.when(r == 1)
        def _():
            shared(k - 1, (0,))

            @pl.when(k > 1)
            def _():
                shared(k - 1, (1,))

        way = lax.rem(r + 1, 2)
        far = lax.rem(z + NZ + jnp.where(way == 0, 1 - k, k - 1), NZ)

        @pl.when((r >= 1) & ((way == 0) | (k > 1)))
        def _():
            compute(far, (r - 1) // 2)

        return carry

    share(0, (0,))
    lax.fori_loop(0, 20, tick, 0)
    share(4, (0,))
    shared(4, (0,))

    def last(yy, carry):
        compute(slab(4, 0), yy)
        return carry

    lax.fori_loop(0, 2, last, 0)

    def finish(group, att_out, lse_out):
        for h in range(4):
            acc = acc_ref[group + h]
            m = m_ref[group + h]
            total = acc[HALF:HALF + 1]
            lse = m + jnp.log(total)
            lse_out[0, h:h + 1, :] = lse[:, :HALF]
            lse_out[1, h:h + 1, :] = lse[:, HALF:]
            ratio = acc[:HALF] / total
            out = ratio[:, :HALF] - lam_ref[h:h + 1, :] * ratio[:, HALF:]
            scale = lax.rsqrt(jnp.mean(out * out, axis=0, keepdims=True) + NORM_EPS)
            normed = out * scale * gain_ref[...]
            att_out[:, h * HALF:(h + 1) * HALF] = normed.T.astype(jnp.bfloat16)

    for half in (0, 1):
        finish(4 * half, att_ref.at[half], lse_ref.at[half])

    rim_copy.wait()
    rim_out[...] = rim_in[...]
    for d in range(3):
        v_to_y(d).wait_send()
        k_to_y(0, 0, d).wait_send()
    to_sibling(0, 0, c).wait_send()

    def drain(k, carry):
        for way in (0, 1):
            for r in range(5):
                z_msg(k, r, way, 0).wait_send()
            for d in range(3):
                k_to_y(k, way, d).wait_send()
            to_sibling(k, way, c).wait_send()
        return carry

    lax.fori_loop(1, 4, drain, 0)
    for r in range(5):
        z_msg(4, r, 0 if r <= 2 else 1, 0).wait_send()
    for d in range(3):
        k_to_y(4, 0, d).wait_send()
    to_sibling(4, 0, c).wait_send()


def attend(q_own, q_far, keys_own, vt, rim_rows, lam, head_gain):
    bf, f32 = jnp.bfloat16, jnp.float32
    dma = pltpu.SemaphoreType.DMA
    vmem = pl.BlockSpec(memory_space=pltpu.VMEM)
    return pl.pallas_call(
        attention_kernel,
        out_shape=(
            jax.ShapeDtypeStruct((2, HALF, 512), bf),
            jax.ShapeDtypeStruct((2, 2, 4, HALF), f32),
            jax.ShapeDtypeStruct((WINDOW, 512), bf),
        ),
        in_specs=[vmem] * 7,
        out_specs=(vmem,) * 3,
        scratch_shapes=[
            pltpu.VMEM((NZ, NC, 2, NY, ROWS, 128), bf),
            pltpu.VMEM((8, 128, 256), bf),
            pltpu.VMEM((8, 1, 256), f32),
            pltpu.VMEM((8, 144, 256), f32),
            pltpu.VMEM((WINDOW, 512), bf),
            *[pltpu.VMEM((KB, 256), f32)] * NB,
            *[pltpu.VMEM((KB, 256), bf)] * NB,
            *[pltpu.VMEM((1, 256), f32)] * NB,
            dma((2,)),
            dma((2, 5, 3)), dma((2, 5, 3)), dma((3,)), dma((3,)),
            dma((2, 5, 5)), dma((2, 5, 5)), dma((2, 5)), dma((2, 5)),
            dma, dma,
        ],
        compiler_params=pltpu.CompilerParams(
            collective_id=0, has_side_effects=True, vmem_limit_bytes=48 * 2**20
        ),
        cost_estimate=pl.CostEstimate(
            flops=2 * 10**10, bytes_accessed=10**6, transcendentals=2 * 10**7
        ),
        name="attend",
    )(
        q_own, q_far, keys_own, vt, rim_rows,
        jnp.broadcast_to(lam[:, None], (4, HALF)),
        jnp.broadcast_to(head_gain[:, None], (128, HALF)),
    )


def local(
    tokens,
    norm_gain,
    query_weight,
    key_weight,
    value_weight,
    mix_lambda,
    head_gain,
    pool_weight,
    pool_mix,
    pool_scale,
    gate_weight,
    out_weight,
):
    model_width = tokens.shape[1]
    rows = copy_for_each(tokens, "tp").reshape(-1, model_width)
    q_own, q_far, keys_own, vt, pool_in, rim_rows, gates = project(
        rows,
        norm_gain,
        query_weight.reshape(model_width, -1),
        key_weight.reshape(model_width, -1),
        value_weight.reshape(model_width, -1),
        pool_weight.reshape(model_width, -1),
        jnp.transpose(gate_weight, (1, 0, 2)),
    )
    att, lse, rim = attend(q_own, q_far, keys_own, vt, rim_rows, mix_lambda, head_gain)
    mixed = output(att, gates, pool_in, rim, pool_mix[0], pool_scale, out_weight)
    return (mixed, jnp.concatenate([lse[0], lse[1]], axis=2))


def solution(mesh):
    in_specs = (
        P(("sp", "tp"), None),
        P(),
        P(None, "tp", None),
        P(None, "tp", None),
        P(None, "tp", None),
        P("tp"),
        P(),
        P(None, "tp", None),
        P("tp", None, None),
        P("tp", None),
        P(None, None, "tp"),
        P("tp", None),
    )
    out_specs = (P(("sp", "tp"), None), P(None, "tp", "sp"))
    return jax.shard_map(local, mesh=mesh, in_specs=in_specs, out_specs=out_specs, check_vma=False)
```

```python
import functools

import jax
import jax.numpy as jnp
from jax import lax
from jax.experimental import pallas as pl
from jax.experimental.pallas import tpu as pltpu
from jax.sharding import PartitionSpec as P

WINDOW = 16
NORM_EPS = 1e-06
MESH = pl.DeviceIdType.MESH
NEG = -1e30
NZ, NY, NC = 8, 4, 2
LAG, NB = 3, 4
ROWS = 256
HALF = 128
KB = 1024


def copy_for_each(array, axis):
    size = lax.axis_size(axis)
    return lax.all_to_all(
        jnp.broadcast_to(array[None], (size, *array.shape)), axis, 0, 0, tiled=True
    )


def project_kernel(
    tok_ref, gain_ref, wq, wk, wv, wp, wg,
    q_own, q_far, k_ref, vt_ref, pool_ref, rim_ref, gate_ref,
    normed, vq, vk, vv, vp, vg, sems,
):
    copies = [
        pltpu.make_async_copy(src, dst, sems.at[n])
        for n, (src, dst) in enumerate(((wk, vk), (wv, vv), (wq, vq), (wp, vp), (wg, vg)))
    ]
    for copy in copies:
        copy.start()
    gain = gain_ref[...]
    for b in range(0, ROWS, 32):
        x = tok_ref[b:b + 32, :].astype(jnp.float32)
        scale = lax.rsqrt(jnp.mean(x * x, axis=1, keepdims=True) + NORM_EPS)
        normed[b:b + 32, :] = (x * scale * gain).astype(jnp.bfloat16)

    def project(weight):
        return jnp.dot(normed[...], weight, preferred_element_type=jnp.float32)

    copies[0].wait()
    k_ref[...] = project(vk[...]).astype(jnp.bfloat16)
    copies[1].wait()
    v = project(vv[...])
    for b in (0, HALF):
        vt_ref[b:b + HALF, :] = v[b:b + HALF].T.astype(jnp.bfloat16)
    copies[2].wait()
    for h in range(4):
        q = project(vq[:, h * 128:(h + 1) * 128]) * 0.125
        q_own[h] = q[:HALF].T.astype(jnp.bfloat16)
        q_far[h] = q[HALF:].T.astype(jnp.bfloat16)
    copies[3].wait()
    pool_in = project(vp[...]).astype(jnp.bfloat16)
    pool_ref[...] = pool_in
    rim_ref[...] = pool_in[ROWS - WINDOW:]
    copies[4].wait()
    for g in (0, 1):
        gate_ref[g] = project(vg[g]).astype(jnp.bfloat16)


def project(rows, norm_gain, wq, wk, wv, wp, wg):
    bf = jnp.bfloat16
    vmem = pl.BlockSpec(memory_space=pltpu.VMEM)
    anywhere = pl.BlockSpec(memory_space=pl.ANY)
    shape = jax.ShapeDtypeStruct
    return pl.pallas_call(
        project_kernel,
        out_shape=(
            shape((4, 128, HALF), bf), shape((4, 128, HALF), bf),
            shape((ROWS, 128), bf), shape((ROWS, 128), bf),
            shape((ROWS, 512), bf), shape((WINDOW, 512), bf), shape((2, ROWS, 512), bf),
        ),
        in_specs=[vmem, vmem] + [anywhere] * 5,
        out_specs=(vmem,) * 7,
        scratch_shapes=[
            pltpu.VMEM((ROWS, 2048), bf),
            pltpu.VMEM(wq.shape, bf), pltpu.VMEM(wk.shape, bf), pltpu.VMEM(wv.shape, bf),
            pltpu.VMEM(wp.shape, bf), pltpu.VMEM(wg.shape, bf),
            pltpu.SemaphoreType.DMA((5,)),
        ],
        compiler_params=pltpu.CompilerParams(vmem_limit_bytes=50 * 2**20),
        cost_estimate=pl.CostEstimate(
            flops=2 * ROWS * 2048 * 2304, bytes_accessed=10**7, transcendentals=0
        ),
        name="project",
    )(rows, norm_gain[None], wq, wk, wv, wp, wg)


def output_kernel(
    att_ref, gate_ref, pool_ref, rim_ref, mix_ref, scale_ref, weight_ref,
    out_ref,
    merged, part, got, s_sem, r_sem,
):
    x = lax.axis_index("tp")
    peers = [{"tp": lax.rem(x + d, 4)} for d in (1, 2, 3)]
    barrier = pltpu.get_barrier_semaphore()
    for peer in peers:
        pl.semaphore_signal(barrier, inc=1, device_id=peer, device_id_type=MESH)

    f32, bf = jnp.float32, jnp.bfloat16
    for cb in range(0, 512, 128):
        cols = slice(cb, cb + 128)
        own = pool_ref[:, cols].astype(f32)
        rim = jnp.where(lax.axis_index("sp") == 0, 0.0, rim_ref[:, cols].astype(f32))
        sums = jnp.concatenate([rim, own], axis=0)
        picked = sums
        for n, shift in enumerate((1, 2, 4, 8)):
            sums = sums + pltpu.roll(sums, shift, 0)
            picked = jnp.where(x >= n, sums, picked)
        position = lax.axis_index("sp") * ROWS + lax.broadcasted_iota(jnp.int32, (ROWS, 128), 0)
        span = jnp.left_shift(jnp.int32(2), x)
        counts = jnp.minimum(position + 1, span).astype(f32)
        merged[:, cols] = (picked[WINDOW:] / counts - own).astype(bf)
    pool_out = jnp.dot(merged[...], mix_ref[...], preferred_element_type=f32) * scale_ref[...]
    attended = jnp.concatenate([att_ref[0], att_ref[1]], axis=0).astype(f32)
    merged[...] = (
        jax.nn.sigmoid(gate_ref[0].astype(f32)) * attended
        + jax.nn.sigmoid(gate_ref[1].astype(f32)) * pool_out
    ).astype(bf)

    def partial(d):
        first = pl.multiple_of(lax.rem(x + d, 4) * 64, 64)
        return jnp.dot(merged[pl.ds(first, 64), :], weight_ref[...], preferred_element_type=f32)

    def send(d):
        return pltpu.make_async_remote_copy(
            src_ref=part.at[d - 1], dst_ref=got.at[d - 1],
            send_sem=s_sem.at[d - 1], recv_sem=r_sem.at[d - 1],
            device_id=peers[d - 1], device_id_type=MESH,
        )

    part[1] = partial(2).astype(bf)
    pl.semaphore_wait(barrier, 3)
    part[0] = partial(1).astype(bf)
    send(2).start()
    part[2] = partial(3).astype(bf)
    send(1).start()
    total = partial(0).astype(bf).astype(f32)
    send(3).start()
    for d in (1, 3, 2):
        send(d).wait()
        total = total + got[d - 1].astype(f32)
    out_ref[...] = total.astype(bf)


def output(att, gates, pool_in, rim, mix, scale, weight):
    bf = jnp.bfloat16
    vmem = pl.BlockSpec(memory_space=pltpu.VMEM)
    dma = pltpu.SemaphoreType.DMA
    return pl.pallas_call(
        output_kernel,
        out_shape=jax.ShapeDtypeStruct((64, 2048), bf),
        in_specs=[vmem] * 7,
        out_specs=vmem,
        scratch_shapes=[
            pltpu.VMEM((ROWS, 512), bf),
            pltpu.VMEM((3, 64, 2048), bf),
            pltpu.VMEM((3, 64, 2048), bf),
            dma((3,)), dma((3,)),
        ],
        compiler_params=pltpu.CompilerParams(
            collective_id=1, has_side_effects=True, vmem_limit_bytes=32 * 2**20
        ),
        name="output",
    )(att, gates, pool_in, rim, mix, scale, weight)


def attention_kernel(
    q_ref, qs_ref, k_ref, v_ref, rim_ref, lam_ref, gain_ref,
    att_ref, lse_ref, rim_out,
    kv, qbd, m_ref, acc_ref, rim_in,
    *rest,
):
    sb, pb, bm = rest[:NB], rest[NB:2 * NB], rest[2 * NB:3 * NB]
    (own_sem, y_s, y_r, vy_s, vy_r, z_s, z_r,
     sib_s, sib_r, rim_s, rim_r) = rest[3 * NB:]
    me = lax.axis_index("sp")
    z, y, c = me // (NY * NC), (me // NC) % NY, me % NC

    def at(zz, yy, cc):
        return {"sp": (zz * NY + yy) * NC + cc}

    sibling = at(z, y, 1 - c)
    z_next = [at((z + 1) % NZ, y, c), at((z + NZ - 1) % NZ, y, c)]
    y_peers = [at(z, (y + d) % NY, c) for d in (1, 2, 3)]

    barrier = pltpu.get_barrier_semaphore()
    n_sp = NZ * NY * NC
    after, before = {"sp": lax.rem(me + 1, n_sp)}, {"sp": lax.rem(me + n_sp - 1, n_sp)}
    peers = [sibling, *z_next, *y_peers, after, before]
    for peer in peers:
        pl.semaphore_signal(barrier, inc=1, device_id=peer, device_id_type=MESH)
    pl.semaphore_wait(barrier, len(peers))

    def remote(src, dst, s, r, dev):
        return pltpu.make_async_remote_copy(
            src_ref=src, dst_ref=dst, send_sem=s, recv_sem=r,
            device_id=dev, device_id_type=MESH,
        )

    def slab(k, way):
        return lax.rem(z + NZ + (k if way else -k), NZ)

    def k_to_y(k, way, d):
        piece = kv.at[slab(k, way), c, 0, y]
        return remote(piece, piece, y_s.at[way, k, d], y_r.at[way, k, d], y_peers[d])

    def k_from_y(k, way, d):
        piece = kv.at[slab(k, way), c, 0, lax.rem(y + NY - (d + 1), NY)]
        return remote(piece, piece, y_s.at[way, k, d], y_r.at[way, k, d], y_peers[d])

    def v_to_y(d):
        return remote(v_ref, kv.at[z, c, 1, y], vy_s.at[d], vy_r.at[d], y_peers[d])

    def v_from_y(d):
        yy = lax.rem(y + NY - (d + 1), NY)
        return remote(v_ref, kv.at[z, c, 1, yy], vy_s.at[d], vy_r.at[d], y_peers[d])

    def z_piece(zs, r):
        kind = jnp.minimum(r, 1)
        return kv.at[zs, c, kind, lax.rem(y + jnp.maximum(r - 1, 0), NY)]

    def z_msg(k, r, way, src_k, src=None):
        piece = z_piece(slab(src_k, way), r)
        return remote(
            piece if src is None else src, piece,
            z_s.at[way, k, r], z_r.at[way, k, r], z_next[way],
        )

    def to_sibling(k, way, cc):
        part = kv.at[slab(k, way), cc]
        return remote(part, part, sib_s.at[way, k], sib_r.at[way, k], sibling)

    own_k = pltpu.make_async_copy(k_ref, kv.at[z, c, 0, y], own_sem.at[0])
    own_v = pltpu.make_async_copy(v_ref, kv.at[z, c, 1, y], own_sem.at[1])
    own_k.start()
    own_v.start()
    for d in (0, 2, 1):
        v_to_y(d).start()
    for way in (0, 1):
        z_msg(1, 0, way, 0, k_ref).start()
        z_msg(1, 1, way, 0, v_ref).start()
    rim_copy = remote(rim_ref, rim_in, rim_s, rim_r, after)
    rim_copy.start()
    own_k.wait()
    for d in (0, 2, 1):
        k_to_y(0, 0, d).start()
    own_v.wait()

    m_ref[...] = jnp.full_like(m_ref, NEG)
    acc_ref[...] = jnp.zeros_like(acc_ref)

    def block_diagonal(q):
        top = lax.broadcasted_iota(jnp.int32, (HALF, HALF), 0) < 64
        zero = jnp.zeros_like(q)
        return jnp.concatenate([jnp.where(top, q, zero), jnp.where(top, zero, q)], axis=1)

    for h in range(4):
        qbd[h] = block_diagonal(q_ref[h])
        qbd[4 + h] = block_diagonal(qs_ref[h])

    for r in (2, 4, 3):
        v_from_y(NY - r).wait_recv()
        for way in (0, 1):
            z_msg(1, r, way, 0).start()

    mine = (z * NY + y) // 2

    ones = jnp.ones((16, KB), jnp.bfloat16)

    def pieces(i, kind):
        zs, yy = i // 2, 2 * lax.rem(i, 2)
        return [kv[zs, cc, kind, yy + d] for d in (0, 1) for cc in (0, 1)]

    def keys(i):
        return jnp.concatenate(pieces(i, 0), axis=0)

    def values(i):
        halves = [v[a:a + HALF] for v in pieces(i, 1) for a in (0, HALF)]
        return jnp.concatenate([jnp.concatenate(halves, axis=1), ones], axis=0)

    def scores(i, t, slot, masked=False):
        s = jnp.dot(keys(i), qbd[t], preferred_element_type=jnp.float32)
        if masked:
            base = me * ROWS + t // 4 * HALF
            key_pos = i * KB + lax.broadcasted_iota(jnp.int32, (KB, 2 * HALF), 0)
            row = lax.broadcasted_iota(jnp.int32, (KB, 2 * HALF), 1)
            row_pos = base + jnp.where(row < HALF, row, row - HALF)
            s = jnp.where(key_pos <= row_pos, s, NEG)
        sb[slot][...] = s
        bm[slot][...] = jnp.max(s, axis=0, keepdims=True)

    def weigh(i, t, slot):
        old = m_ref[t]
        new = jnp.maximum(old, bm[slot][...])
        m_ref[t] = new
        pb[slot][...] = jnp.exp(sb[slot][...] - new).astype(jnp.bfloat16)
        acc_ref[t] = acc_ref[t] * jnp.exp(old - new) + jnp.dot(
            values(i), pb[slot][...], preferred_element_type=jnp.float32
        )

    def block(items, masked=False):
        n = len(items)
        for u in range(LAG):
            scores(*items[u], u % NB, masked)
        for u in range(n):
            if u + LAG < n:
                scores(*items[u + LAG], (u + LAG) % NB, masked)
            weigh(*items[u], u % NB)

    def compute(zs, half):
        i = 2 * zs + half

        @pl.when(i < mine)
        def _():
            block([(i, t) for t in range(8)])

        @pl.when(i == mine)
        def _():
            block([(i, t) for t in range(8)], True)

    def share(k, ways):
        for way in ways:
            for d in range(3):
                k_from_y(k, way, d).wait_recv()
            to_sibling(k, way, c).start()

    def shared(k, ways):
        for way in ways:
            to_sibling(k, way, 1 - c).wait_recv()

    def serve(k, r, way, forward):
        z_msg(k, r, way, k).wait_recv()
        if forward is not None:
            @pl.when(forward)
            def _():
                z_msg(k + 1, r, way, k).start()

        @pl.when(r == 0)
        def _():
            for d in (0, 2, 1):
                k_to_y(k, way, d).start()

    def both(k, r):
        serve(k, r, 0, (k < 3) | (r <= 2))
        serve(k, r, 1, (k < 3) | (r >= 3))

    def tick(n, carry):
        k, r = n // 5 + 1, lax.rem(n, 5)

        @pl.when(k <= 3)
        def _():
            both(k, r)

        @pl.when((k == 4) & (r <= 2))
        def _():
            serve(k, r, 0, None)

        @pl.when((k == 4) & (r <= 1))
        def _():
            z_msg(k, r + 3, 1, k).wait_recv()

        @pl.when((r == 4) & (k <= 3))
        def _():
            share(k, (0, 1))

        @pl.when((r == 3) & (k == 4))
        def _():
            share(4, (0,))

        @pl.when(r == 1)
        def _():
            shared(k - 1, (0,))

            @pl.when(k > 1)
            def _():
                shared(k - 1, (1,))

        way = lax.rem(r + 1, 2)
        far = lax.rem(z + NZ + jnp.where(way == 0, 1 - k, k - 1), NZ)

        @pl.when((r >= 1) & ((way == 0) | (k > 1)))
        def _():
            compute(far, (r - 1) // 2)

        return carry

    share(0, (0,))
    lax.fori_loop(0, 20, tick, 0)
    shared(4, (0,))

    def last(yy, carry):
        compute(slab(4, 0), yy)
        return carry

    lax.fori_loop(0, 2, last, 0)

    def finish(group, att_out, lse_out):
        for h in range(4):
            acc = acc_ref[group + h]
            m = m_ref[group + h]
            total = acc[HALF:HALF + 1]
            lse = m + jnp.log(total)
            lse_out[0, h:h + 1, :] = lse[:, :HALF]
            lse_out[1, h:h + 1, :] = lse[:, HALF:]
            ratio = acc[:HALF] / total
            out = ratio[:, :HALF] - lam_ref[h:h + 1, :] * ratio[:, HALF:]
            scale = lax.rsqrt(jnp.mean(out * out, axis=0, keepdims=True) + NORM_EPS)
            normed = out * scale * gain_ref[...]
            att_out[:, h * HALF:(h + 1) * HALF] = normed.T.astype(jnp.bfloat16)

    for half in (0, 1):
        finish(4 * half, att_ref.at[half], lse_ref.at[half])

    rim_copy.wait()
    rim_out[...] = rim_in[...]
    for d in range(3):
        v_to_y(d).wait_send()
        k_to_y(0, 0, d).wait_send()
    to_sibling(0, 0, c).wait_send()

    def drain(k, carry):
        for way in (0, 1):
            for r in range(5):
                z_msg(k, r, way, 0).wait_send()
            for d in range(3):
                k_to_y(k, way, d).wait_send()
            to_sibling(k, way, c).wait_send()
        return carry

    lax.fori_loop(1, 4, drain, 0)
    for r in range(5):
        z_msg(4, r, 0 if r <= 2 else 1, 0).wait_send()
    for d in range(3):
        k_to_y(4, 0, d).wait_send()
    to_sibling(4, 0, c).wait_send()


def attend(q_own, q_far, keys_own, vt, rim_rows, lam, head_gain):
    bf, f32 = jnp.bfloat16, jnp.float32
    dma = pltpu.SemaphoreType.DMA
    vmem = pl.BlockSpec(memory_space=pltpu.VMEM)
    return pl.pallas_call(
        attention_kernel,
        out_shape=(
            jax.ShapeDtypeStruct((2, HALF, 512), bf),
            jax.ShapeDtypeStruct((2, 2, 4, HALF), f32),
            jax.ShapeDtypeStruct((WINDOW, 512), bf),
        ),
        in_specs=[vmem] * 7,
        out_specs=(vmem,) * 3,
        scratch_shapes=[
            pltpu.VMEM((NZ, NC, 2, NY, ROWS, 128), bf),
            pltpu.VMEM((8, 128, 256), bf),
            pltpu.VMEM((8, 1, 256), f32),
            pltpu.VMEM((8, 144, 256), f32),
            pltpu.VMEM((WINDOW, 512), bf),
            *[pltpu.VMEM((KB, 256), f32)] * NB,
            *[pltpu.VMEM((KB, 256), bf)] * NB,
            *[pltpu.VMEM((1, 256), f32)] * NB,
            dma((2,)),
            dma((2, 5, 3)), dma((2, 5, 3)), dma((3,)), dma((3,)),
            dma((2, 5, 5)), dma((2, 5, 5)), dma((2, 5)), dma((2, 5)),
            dma, dma,
        ],
        compiler_params=pltpu.CompilerParams(
            collective_id=0, has_side_effects=True, vmem_limit_bytes=48 * 2**20
        ),
        cost_estimate=pl.CostEstimate(
            flops=2 * 10**10, bytes_accessed=10**6, transcendentals=2 * 10**7
        ),
        name="attend",
    )(
        q_own, q_far, keys_own, vt, rim_rows,
        jnp.broadcast_to(lam[:, None], (4, HALF)),
        jnp.broadcast_to(head_gain[:, None], (128, HALF)),
    )


def local(
    tokens,
    norm_gain,
    query_weight,
    key_weight,
    value_weight,
    mix_lambda,
    head_gain,
    pool_weight,
    pool_mix,
    pool_scale,
    gate_weight,
    out_weight,
):
    model_width = tokens.shape[1]
    rows = copy_for_each(tokens, "tp").reshape(-1, model_width)
    q_own, q_far, keys_own, vt, pool_in, rim_rows, gates = project(
        rows,
        norm_gain,
        query_weight.reshape(model_width, -1),
        key_weight.reshape(model_width, -1),
        value_weight.reshape(model_width, -1),
        pool_weight.reshape(model_width, -1),
        jnp.transpose(gate_weight, (1, 0, 2)),
    )
    att, lse, rim = attend(q_own, q_far, keys_own, vt, rim_rows, mix_lambda, head_gain)
    mixed = output(att, gates, pool_in, rim, pool_mix[0], pool_scale, out_weight)
    return (mixed, jnp.concatenate([lse[0], lse[1]], axis=2))


def solution(mesh):
    in_specs = (
        P(("sp", "tp"), None),
        P(),
        P(None, "tp", None),
        P(None, "tp", None),
        P(None, "tp", None),
        P("tp"),
        P(),
        P(None, "tp", None),
        P("tp", None, None),
        P("tp", None),
        P(None, None, "tp"),
        P("tp", None),
    )
    out_specs = (P(("sp", "tp"), None), P(None, "tp", "sp"))
    return jax.shard_map(local, mesh=mesh, in_specs=in_specs, out_specs=out_specs, check_vma=False)
```

```python
import functools

import jax
import jax.numpy as jnp
from jax import lax
from jax.experimental import pallas as pl
from jax.experimental.pallas import tpu as pltpu
from jax.sharding import PartitionSpec as P

WINDOW = 16
NORM_EPS = 1e-06
MESH = pl.DeviceIdType.MESH
NEG = -1e30
NZ, NY, NC = 8, 4, 2
LAG, NB = 3, 4
ROWS = 256
HALF = 128
KB = 1024


def copy_for_each(array, axis):
    size = lax.axis_size(axis)
    return lax.all_to_all(
        jnp.broadcast_to(array[None], (size, *array.shape)), axis, 0, 0, tiled=True
    )


def project_kernel(
    tok_ref, gain_ref, wq, wk, wv, wp, wg,
    q_own, q_far, k_ref, vt_ref, pool_ref, rim_ref, gate_ref,
    normed, vq, vk, vv, vp, vg, sems,
):
    copies = [
        pltpu.make_async_copy(src, dst, sems.at[n])
        for n, (src, dst) in enumerate(((wk, vk), (wv, vv), (wq, vq), (wp, vp), (wg, vg)))
    ]
    for copy in copies:
        copy.start()
    gain = gain_ref[...]
    for b in range(0, ROWS, 32):
        x = tok_ref[b:b + 32, :].astype(jnp.float32)
        scale = lax.rsqrt(jnp.mean(x * x, axis=1, keepdims=True) + NORM_EPS)
        normed[b:b + 32, :] = (x * scale * gain).astype(jnp.bfloat16)

    def project(weight):
        return jnp.dot(normed[...], weight, preferred_element_type=jnp.float32)

    copies[0].wait()
    k_ref[...] = project(vk[...]).astype(jnp.bfloat16)
    copies[1].wait()
    v = project(vv[...])
    for b in (0, HALF):
        vt_ref[b:b + HALF, :] = v[b:b + HALF].T.astype(jnp.bfloat16)
    copies[2].wait()
    for h in range(4):
        q = project(vq[:, h * 128:(h + 1) * 128]) * 0.125
        q_own[h] = q[:HALF].T.astype(jnp.bfloat16)
        q_far[h] = q[HALF:].T.astype(jnp.bfloat16)
    copies[3].wait()
    pool_in = project(vp[...]).astype(jnp.bfloat16)
    pool_ref[...] = pool_in
    rim_ref[...] = pool_in[ROWS - WINDOW:]
    copies[4].wait()
    for g in (0, 1):
        gate_ref[g] = project(vg[g]).astype(jnp.bfloat16)


def project(rows, norm_gain, wq, wk, wv, wp, wg):
    bf = jnp.bfloat16
    vmem = pl.BlockSpec(memory_space=pltpu.VMEM)
    anywhere = pl.BlockSpec(memory_space=pl.ANY)
    shape = jax.ShapeDtypeStruct
    return pl.pallas_call(
        project_kernel,
        out_shape=(
            shape((4, 128, HALF), bf), shape((4, 128, HALF), bf),
            shape((ROWS, 128), bf), shape((ROWS, 128), bf),
            shape((ROWS, 512), bf), shape((WINDOW, 512), bf), shape((2, ROWS, 512), bf),
        ),
        in_specs=[vmem, vmem] + [anywhere] * 5,
        out_specs=(vmem,) * 7,
        scratch_shapes=[
            pltpu.VMEM((ROWS, 2048), bf),
            pltpu.VMEM(wq.shape, bf), pltpu.VMEM(wk.shape, bf), pltpu.VMEM(wv.shape, bf),
            pltpu.VMEM(wp.shape, bf), pltpu.VMEM(wg.shape, bf),
            pltpu.SemaphoreType.DMA((5,)),
        ],
        compiler_params=pltpu.CompilerParams(vmem_limit_bytes=50 * 2**20),
        cost_estimate=pl.CostEstimate(
            flops=2 * ROWS * 2048 * 2304, bytes_accessed=10**7, transcendentals=0
        ),
        name="project",
    )(rows, norm_gain[None], wq, wk, wv, wp, wg)


def output_kernel(
    att_ref, gate_ref, pool_ref, rim_ref, mix_ref, scale_ref, weight_ref,
    out_ref,
    merged, part, got, s_sem, r_sem,
):
    x = lax.axis_index("tp")
    peers = [{"tp": lax.rem(x + d, 4)} for d in (1, 2, 3)]
    barrier = pltpu.get_barrier_semaphore()
    for peer in peers:
        pl.semaphore_signal(barrier, inc=1, device_id=peer, device_id_type=MESH)

    f32, bf = jnp.float32, jnp.bfloat16
    for cb in range(0, 512, 128):
        cols = slice(cb, cb + 128)
        own = pool_ref[:, cols].astype(f32)
        rim = jnp.where(lax.axis_index("sp") == 0, 0.0, rim_ref[:, cols].astype(f32))
        sums = jnp.concatenate([rim, own], axis=0)
        picked = sums
        for n, shift in enumerate((1, 2, 4, 8)):
            sums = sums + pltpu.roll(sums, shift, 0)
            picked = jnp.where(x >= n, sums, picked)
        position = lax.axis_index("sp") * ROWS + lax.broadcasted_iota(jnp.int32, (ROWS, 128), 0)
        span = jnp.left_shift(jnp.int32(2), x)
        counts = jnp.minimum(position + 1, span).astype(f32)
        merged[:, cols] = (picked[WINDOW:] / counts - own).astype(bf)
    pool_out = jnp.dot(merged[...], mix_ref[...], preferred_element_type=f32) * scale_ref[...]
    attended = jnp.concatenate([att_ref[0], att_ref[1]], axis=0).astype(f32)
    merged[...] = (
        jax.nn.sigmoid(gate_ref[0].astype(f32)) * attended
        + jax.nn.sigmoid(gate_ref[1].astype(f32)) * pool_out
    ).astype(bf)

    def partial(d):
        first = pl.multiple_of(lax.rem(x + d, 4) * 64, 64)
        return jnp.dot(merged[pl.ds(first, 64), :], weight_ref[...], preferred_element_type=f32)

    def send(d):
        return pltpu.make_async_remote_copy(
            src_ref=part.at[d - 1], dst_ref=got.at[d - 1],
            send_sem=s_sem.at[d - 1], recv_sem=r_sem.at[d - 1],
            device_id=peers[d - 1], device_id_type=MESH,
        )

    part[1] = partial(2).astype(bf)
    pl.semaphore_wait(barrier, 3)
    part[0] = partial(1).astype(bf)
    send(2).start()
    part[2] = partial(3).astype(bf)
    send(1).start()
    total = partial(0).astype(bf).astype(f32)
    send(3).start()
    for d in (1, 3, 2):
        send(d).wait()
        total = total + got[d - 1].astype(f32)
    out_ref[...] = total.astype(bf)


def output(att, gates, pool_in, rim, mix, scale, weight):
    bf = jnp.bfloat16
    vmem = pl.BlockSpec(memory_space=pltpu.VMEM)
    dma = pltpu.SemaphoreType.DMA
    return pl.pallas_call(
        output_kernel,
        out_shape=jax.ShapeDtypeStruct((64, 2048), bf),
        in_specs=[vmem] * 7,
        out_specs=vmem,
        scratch_shapes=[
            pltpu.VMEM((ROWS, 512), bf),
            pltpu.VMEM((3, 64, 2048), bf),
            pltpu.VMEM((3, 64, 2048), bf),
            dma((3,)), dma((3,)),
        ],
        compiler_params=pltpu.CompilerParams(
            collective_id=1, has_side_effects=True, vmem_limit_bytes=32 * 2**20
        ),
        name="output",
    )(att, gates, pool_in, rim, mix, scale, weight)


def attention_kernel(
    q_ref, qs_ref, k_ref, v_ref, rim_ref, lam_ref, gain_ref,
    att_ref, lse_ref, rim_out,
    kv, qbd, m_ref, acc_ref, rim_in,
    *rest,
):
    sb, pb, bm = rest[:NB], rest[NB:2 * NB], rest[2 * NB:3 * NB]
    (own_sem, y_s, y_r, vy_s, vy_r, z_s, z_r,
     sib_s, sib_r, rim_s, rim_r) = rest[3 * NB:]
    me = lax.axis_index("sp")
    z, y, c = me // (NY * NC), (me // NC) % NY, me % NC

    def at(zz, yy, cc):
        return {"sp": (zz * NY + yy) * NC + cc}

    sibling = at(z, y, 1 - c)
    z_next = [at((z + 1) % NZ, y, c), at((z + NZ - 1) % NZ, y, c)]
    y_peers = [at(z, (y + d) % NY, c) for d in (1, 2, 3)]

    barrier = pltpu.get_barrier_semaphore()
    n_sp = NZ * NY * NC
    after, before = {"sp": lax.rem(me + 1, n_sp)}, {"sp": lax.rem(me + n_sp - 1, n_sp)}
    peers = [sibling, *z_next, *y_peers, after, before]
    for peer in peers:
        pl.semaphore_signal(barrier, inc=1, device_id=peer, device_id_type=MESH)
    pl.semaphore_wait(barrier, len(peers))

    def remote(src, dst, s, r, dev):
        return pltpu.make_async_remote_copy(
            src_ref=src, dst_ref=dst, send_sem=s, recv_sem=r,
            device_id=dev, device_id_type=MESH,
        )

    def slab(k, way):
        return lax.rem(z + NZ + (k if way else -k), NZ)

    def k_to_y(k, way, d):
        piece = kv.at[slab(k, way), c, 0, y]
        return remote(piece, piece, y_s.at[way, k, d], y_r.at[way, k, d], y_peers[d])

    def k_from_y(k, way, d):
        piece = kv.at[slab(k, way), c, 0, lax.rem(y + NY - (d + 1), NY)]
        return remote(piece, piece, y_s.at[way, k, d], y_r.at[way, k, d], y_peers[d])

    def v_to_y(d):
        return remote(v_ref, kv.at[z, c, 1, y], vy_s.at[d], vy_r.at[d], y_peers[d])

    def v_from_y(d):
        yy = lax.rem(y + NY - (d + 1), NY)
        return remote(v_ref, kv.at[z, c, 1, yy], vy_s.at[d], vy_r.at[d], y_peers[d])

    def z_piece(zs, r):
        kind = jnp.minimum(r, 1)
        return kv.at[zs, c, kind, lax.rem(y + jnp.maximum(r - 1, 0), NY)]

    def z_msg(k, r, way, src_k, src=None):
        piece = z_piece(slab(src_k, way), r)
        return remote(
            piece if src is None else src, piece,
            z_s.at[way, k, r], z_r.at[way, k, r], z_next[way],
        )

    def to_sibling(k, way, cc):
        part = kv.at[slab(k, way), cc]
        return remote(part, part, sib_s.at[way, k], sib_r.at[way, k], sibling)

    own_k = pltpu.make_async_copy(k_ref, kv.at[z, c, 0, y], own_sem.at[0])
    own_v = pltpu.make_async_copy(v_ref, kv.at[z, c, 1, y], own_sem.at[1])
    own_k.start()
    own_v.start()
    for d in (0, 2, 1):
        v_to_y(d).start()
    for way in (0, 1):
        z_msg(1, 0, way, 0, k_ref).start()
        z_msg(1, 1, way, 0, v_ref).start()
    rim_copy = remote(rim_ref, rim_in, rim_s, rim_r, after)
    rim_copy.start()
    own_k.wait()
    for d in (0, 2, 1):
        k_to_y(0, 0, d).start()
    own_v.wait()

    m_ref[...] = jnp.full_like(m_ref, NEG)
    acc_ref[...] = jnp.zeros_like(acc_ref)

    def block_diagonal(q):
        top = lax.broadcasted_iota(jnp.int32, (HALF, HALF), 0) < 64
        zero = jnp.zeros_like(q)
        return jnp.concatenate([jnp.where(top, q, zero), jnp.where(top, zero, q)], axis=1)

    for h in range(4):
        qbd[h] = block_diagonal(q_ref[h])
        qbd[4 + h] = block_diagonal(qs_ref[h])

    for r in (2, 4, 3):
        v_from_y(NY - r).wait_recv()
        for way in (0, 1):
            z_msg(1, r, way, 0).start()

    mine = (z * NY + y) // 2

    ones = jnp.ones((16, KB), jnp.bfloat16)

    def pieces(i, kind):
        zs, yy = i // 2, 2 * lax.rem(i, 2)
        return [kv[zs, cc, kind, yy + d] for d in (0, 1) for cc in (0, 1)]

    def keys(i):
        return jnp.concatenate(pieces(i, 0), axis=0)

    def values(i):
        halves = [v[a:a + HALF] for v in pieces(i, 1) for a in (0, HALF)]
        return jnp.concatenate([jnp.concatenate(halves, axis=1), ones], axis=0)

    def scores(i, t, slot, masked=False):
        s = jnp.dot(keys(i), qbd[t], preferred_element_type=jnp.float32)
        if masked:
            base = me * ROWS + t // 4 * HALF
            key_pos = i * KB + lax.broadcasted_iota(jnp.int32, (KB, 2 * HALF), 0)
            row = lax.broadcasted_iota(jnp.int32, (KB, 2 * HALF), 1)
            row_pos = base + jnp.where(row < HALF, row, row - HALF)
            s = jnp.where(key_pos <= row_pos, s, NEG)
        sb[slot][...] = s
        bm[slot][...] = jnp.max(s, axis=0, keepdims=True)

    def weigh(i, t, slot):
        old = m_ref[t]
        new = jnp.maximum(old, bm[slot][...])
        m_ref[t] = new
        pb[slot][...] = jnp.exp(sb[slot][...] - new).astype(jnp.bfloat16)
        acc_ref[t] = acc_ref[t] * jnp.exp(old - new) + jnp.dot(
            values(i), pb[slot][...], preferred_element_type=jnp.float32
        )

    def block(items, masked=False):
        n = len(items)
        for u in range(LAG):
            scores(*items[u], u % NB, masked)
        for u in range(n):
            if u + LAG < n:
                scores(*items[u + LAG], (u + LAG) % NB, masked)
            weigh(*items[u], u % NB)

    def compute(zs, half):
        i = 2 * zs + half

        @pl.when(i < mine)
        def _():
            block([(i, t) for t in range(8)])

        @pl.when(i == mine)
        def _():
            block([(i, t) for t in range(8)], True)

    def share(k, ways):
        for way in ways:
            for d in range(3):
                k_from_y(k, way, d).wait_recv()
            to_sibling(k, way, c).start()

    def shared(k, ways):
        for way in ways:
            to_sibling(k, way, 1 - c).wait_recv()

    def serve(k, r, way, forward):
        z_msg(k, r, way, k).wait_recv()
        if forward is not None:
            @pl.when(forward)
            def _():
                z_msg(k + 1, r, way, k).start()

        @pl.when(r == 0)
        def _():
            for d in (0, 2, 1):
                k_to_y(k, way, d).start()

    def both(k, r):
        serve(k, r, 0, (k < 3) | (r <= 2))
        serve(k, r, 1, (k < 3) | (r >= 3))

    def tick(n, carry):
        k, r = n // 5 + 1, lax.rem(n, 5)

        @pl.when(k <= 3)
        def _():
            both(k, r)

        @pl.when((k == 4) & (r <= 2))
        def _():
            serve(k, r, 0, None)

        @pl.when((k == 4) & (r <= 1))
        def _():
            z_msg(k, r + 3, 1, k).wait_recv()

        @pl.when((r == 4) & (k <= 3))
        def _():
            share(k, (0, 1))

        @pl.when((r == 3) & (k == 4))
        def _():
            share(4, (0,))

        @pl.when((r == 0) & (k == 1))
        def _():
            share(0, (0,))

        @pl.when(r == 1)
        def _():
            shared(k - 1, (0,))

            @pl.when(k > 1)
            def _():
                shared(k - 1, (1,))

        way = lax.rem(r + 1, 2)
        far = lax.rem(z + NZ + jnp.where(way == 0, 1 - k, k - 1), NZ)

        @pl.when((r >= 1) & ((way == 0) | (k > 1)))
        def _():
            compute(far, (r - 1) // 2)

        return carry

    lax.fori_loop(0, 20, tick, 0)
    shared(4, (0,))

    def last(yy, carry):
        compute(slab(4, 0), yy)
        return carry

    lax.fori_loop(0, 2, last, 0)

    def finish(group, att_out, lse_out):
        for h in range(4):
            acc = acc_ref[group + h]
            m = m_ref[group + h]
            total = acc[HALF:HALF + 1]
            lse = m + jnp.log(total)
            lse_out[0, h:h + 1, :] = lse[:, :HALF]
            lse_out[1, h:h + 1, :] = lse[:, HALF:]
            ratio = acc[:HALF] / total
            out = ratio[:, :HALF] - lam_ref[h:h + 1, :] * ratio[:, HALF:]
            scale = lax.rsqrt(jnp.mean(out * out, axis=0, keepdims=True) + NORM_EPS)
            normed = out * scale * gain_ref[...]
            att_out[:, h * HALF:(h + 1) * HALF] = normed.T.astype(jnp.bfloat16)

    for half in (0, 1):
        finish(4 * half, att_ref.at[half], lse_ref.at[half])

    rim_copy.wait()
    rim_out[...] = rim_in[...]
    for d in range(3):
        v_to_y(d).wait_send()
        k_to_y(0, 0, d).wait_send()
    to_sibling(0, 0, c).wait_send()

    def drain(k, carry):
        for way in (0, 1):
            for r in range(5):
                z_msg(k, r, way, 0).wait_send()
            for d in range(3):
                k_to_y(k, way, d).wait_send()
            to_sibling(k, way, c).wait_send()
        return carry

    lax.fori_loop(1, 4, drain, 0)
    for r in range(5):
        z_msg(4, r, 0 if r <= 2 else 1, 0).wait_send()
    for d in range(3):
        k_to_y(4, 0, d).wait_send()
    to_sibling(4, 0, c).wait_send()


def attend(q_own, q_far, keys_own, vt, rim_rows, lam, head_gain):
    bf, f32 = jnp.bfloat16, jnp.float32
    dma = pltpu.SemaphoreType.DMA
    vmem = pl.BlockSpec(memory_space=pltpu.VMEM)
    return pl.pallas_call(
        attention_kernel,
        out_shape=(
            jax.ShapeDtypeStruct((2, HALF, 512), bf),
            jax.ShapeDtypeStruct((2, 2, 4, HALF), f32),
            jax.ShapeDtypeStruct((WINDOW, 512), bf),
        ),
        in_specs=[vmem] * 7,
        out_specs=(vmem,) * 3,
        scratch_shapes=[
            pltpu.VMEM((NZ, NC, 2, NY, ROWS, 128), bf),
            pltpu.VMEM((8, 128, 256), bf),
            pltpu.VMEM((8, 1, 256), f32),
            pltpu.VMEM((8, 144, 256), f32),
            pltpu.VMEM((WINDOW, 512), bf),
            *[pltpu.VMEM((KB, 256), f32)] * NB,
            *[pltpu.VMEM((KB, 256), bf)] * NB,
            *[pltpu.VMEM((1, 256), f32)] * NB,
            dma((2,)),
            dma((2, 5, 3)), dma((2, 5, 3)), dma((3,)), dma((3,)),
            dma((2, 5, 5)), dma((2, 5, 5)), dma((2, 5)), dma((2, 5)),
            dma, dma,
        ],
        compiler_params=pltpu.CompilerParams(
            collective_id=0, has_side_effects=True, vmem_limit_bytes=48 * 2**20
        ),
        cost_estimate=pl.CostEstimate(
            flops=2 * 10**10, bytes_accessed=10**6, transcendentals=2 * 10**7
        ),
        name="attend",
    )(
        q_own, q_far, keys_own, vt, rim_rows,
        jnp.broadcast_to(lam[:, None], (4, HALF)),
        jnp.broadcast_to(head_gain[:, None], (128, HALF)),
    )


def local(
    tokens,
    norm_gain,
    query_weight,
    key_weight,
    value_weight,
    mix_lambda,
    head_gain,
    pool_weight,
    pool_mix,
    pool_scale,
    gate_weight,
    out_weight,
):
    model_width = tokens.shape[1]
    rows = copy_for_each(tokens, "tp").reshape(-1, model_width)
    q_own, q_far, keys_own, vt, pool_in, rim_rows, gates = project(
        rows,
        norm_gain,
        query_weight.reshape(model_width, -1),
        key_weight.reshape(model_width, -1),
        value_weight.reshape(model_width, -1),
        pool_weight.reshape(model_width, -1),
        jnp.transpose(gate_weight, (1, 0, 2)),
    )
    att, lse, rim = attend(q_own, q_far, keys_own, vt, rim_rows, mix_lambda, head_gain)
    mixed = output(att, gates, pool_in, rim, pool_mix[0], pool_scale, out_weight)
    return (mixed, jnp.concatenate([lse[0], lse[1]], axis=2))


def solution(mesh):
    in_specs = (
        P(("sp", "tp"), None),
        P(),
        P(None, "tp", None),
        P(None, "tp", None),
        P(None, "tp", None),
        P("tp"),
        P(),
        P(None, "tp", None),
        P("tp", None, None),
        P("tp", None),
        P(None, None, "tp"),
        P("tp", None),
    )
    out_specs = (P(("sp", "tp"), None), P(None, "tp", "sp"))
    return jax.shard_map(local, mesh=mesh, in_specs=in_specs, out_specs=out_specs, check_vma=False)
```
